128 devices in a mesh: ep: 32 (over z, y, core), tp: 4 (over x).
Axes of the slice: x: 4, y: 4, z: 4, core: 2. Of those that a mesh axis runs over, the one named last changes fastest.
Arguments:
- mix_in: bfloat16 [16384, 4096], P(('ep', 'tp')), may hold values from -6 to 6
- mix_gain: float32 [4096], replicated, may hold values from 0.1 to 1.9
- proj_b: bfloat16 [4096, 1024], P(None, 'tp'), may hold values from -0.09375 to 0.09375
- proj_c: bfloat16 [4096, 1024], P(None, 'tp'), may hold values from -0.09375 to 0.09375
- proj_h: bfloat16 [4096, 1024], P(None, 'tp'), may hold values from -0.09375 to 0.09375
- conv_taps: bfloat16 [3, 1024], P(None, 'tp'), may hold values from -3.5 to 3.5
- proj_out: bfloat16 [1024, 4096], P('tp'), may hold values from -0.1875 to 0.1875
- moe_in: bfloat16 [16384, 4096], P(('ep', 'tp')), may hold values from -6 to 6
- moe_gain: float32 [4096], replicated, may hold values from 0.1 to 1.9
- routes: int32 [16384, 2], P(('ep', 'tp')), may hold values from 0 to 31, all different within a row; in each aligned block of 128 rows (0 to 127, 128 to 255, ...) at most 14 rows name the same one
- group_logits: float32 [16384, 4], P(('ep', 'tp')), may hold values from -6 to 6
- pair_logits: float32 [16384, 2], P(('ep', 'tp')), may hold values from -6 to 6
- expert_gate: bfloat16 [32, 4096, 2048], P('ep', None, 'tp'), may hold values from -0.09375 to 0.09375
- expert_up: bfloat16 [32, 4096, 2048], P('ep', None, 'tp'), may hold values from -0.09375 to 0.09375
- expert_down: bfloat16 [32, 2048, 4096], P('ep', 'tp'), may hold values from -0.125 to 0.125
Outputs:
- mix_out: bfloat16 [16384, 4096], P(('ep', 'tp'))
- moe_out: bfloat16 [16384, 4096], P(('ep', 'tp'))
The draws below stay inside these ranges and needn't reach their ends.
Inputs may be any that keep to these rules, and one draw needn't show every extreme that they name: `routes`: each row names 2 different experts. Among the 128 rows of one device no expert is named more than 14 times, and in some device's rows some expert is named exactly 14 times.
All inputs are finite; a program needn't handle non-finite values.
Results may differ from the reference program's by a relative error of at most 0.015.
Values may be sent and summed in bfloat16 or wider, within the bound.
A program may use at most 192 MiB of HBM per device.

```python
import math
import jax
import jax.numpy as jnp
import numpy as np
from jax import lax

D = 4096
CONV_CH = 1024
FF = 2048
GROUPS = 4
TOP = 2
TOK_DEV = 128
EXPERTS = 32
EXP_GROUP = 8
CAP = 14
TOKENS = 16384
N_EP = 32
N_TP = 4


def level_of(rng, dims, pieces, smallest, largest):
    def one(axis_at, shards_of):
        steps = jax.random.uniform(jax.random.fold_in(jax.random.fold_in(rng, 6), axis_at), (shards_of,), jnp.float32, smallest / len(pieces), largest / len(pieces))
        return jnp.repeat(jnp.exp(steps), dims[axis_at] // shards_of).reshape((-1,) + (1,) * (len(dims) - axis_at - 1))

    gain = one(*pieces[0])
    for cut in pieces[1:]:
        gain = gain * one(*cut)
    return gain


def assign_block(own_key, own, number, rows, number_of, top, reach, lean):
    sequence = jax.random.permutation(own_key, number_of)
    crowded, common = load_shares(number_of, rows * top, reach, lean, True), load_shares(number_of, rows * top, reach, lean, False)
    places = jnp.arange(number_of)

    def named(tallies, turn):
        used = int((tallies > 0).sum())
        fixed = max(1, used // 4)
        shifted = fixed + (places - fixed + turn * (used - fixed)) % max(1, number_of - fixed)
        return jnp.zeros((number_of,), jnp.int32).at[sequence[jnp.where(places < fixed, places, shifted)]].set(jnp.asarray(tallies, jnp.int32))

    tallies = jnp.where(number % 4 == 0, named(crowded, number // 4), named(common, number - number // 4 - 1))
    mixed = jax.random.permutation(jax.random.fold_in(own, 3), number_of)
    donor, taker = mixed[0:number_of // 2 * 2:2], mixed[1:number_of // 2 * 2:2]
    margin = jnp.minimum(tallies[donor] - 1, reach - tallies[taker]) // 2
    margin = jnp.where((donor == sequence[0]) | (taker == sequence[0]) | (tallies[taker] == 0), 0, jnp.maximum(margin, 0))
    shifted = jax.random.randint(jax.random.fold_in(own, 4), (number_of // 2,), 0, 1 << 20) % (margin + 1)
    tallies = tallies.at[donor].add(-shifted).at[taker].add(shifted)
    members = jnp.searchsorted(jnp.cumsum(tallies), jnp.arange(rows * top), side="right").astype(jnp.int32)
    listing = members.reshape(top, rows).T
    listing = listing[jax.random.permutation(jax.random.fold_in(own, 1), rows)]
    turn = jax.random.randint(jax.random.fold_in(own, 2), (rows, 1), 0, top)
    return jnp.take_along_axis(listing, (jnp.arange(top)[None, :] + turn) % top, axis=1)


def load_shares(number_of, total, most, lean, full):
    portions = [(1 << 20) // math.isqrt(grade ** lean) + 1 for grade in range(1, number_of + 1)]
    largest = most if full else min(most, max(-(-total // number_of), total * portions[0] // sum(portions)))
    least = 1 if total - largest >= number_of - 1 else 0
    given, surplus = [largest] + [least] * (number_of - 1), total - largest - least * (number_of - 1)
    while surplus > 0:
        free = [i for i in range(1, number_of) if given[i] < largest] or [i for i in range(1, number_of) if given[i] < most]
        whole, budget = sum([portions[i] for i in free]), surplus
        for i in free:
            more = min(most - given[i], max(1, budget * portions[i] // whole), surplus)
            given[i] = given[i] + more
            surplus = surplus - more
    return np.array(given)


def centred(stream_key, shape, scale, bound, cuts=(), held_as=jnp.bfloat16):
    drawn = scale * jax.random.normal(stream_key, shape, jnp.float32)
    if cuts:
        drawn = drawn * level_of(stream_key, shape, cuts, -0.22, 0.18)
    return jnp.clip(drawn, -bound, bound).astype(held_as)


def setup_inputs(seed: int = 0) -> dict:
    arg_keys = jax.random.split(jax.random.key(seed), 16)
    mix_in = centred(arg_keys[0], (TOKENS, D), 1.0, 6.0, ((0, 128),))
    mix_gain = jnp.clip(1.0 + 0.18 * jax.random.normal(arg_keys[1], (D,), jnp.float32), 0.1, 1.9)
    proj_b = centred(arg_keys[2], (D, CONV_CH), D ** -0.5, 0.09375, ((1, 4),))
    proj_c = centred(arg_keys[3], (D, CONV_CH), D ** -0.5, 0.09375, ((1, 4),))
    proj_h = centred(arg_keys[4], (D, CONV_CH), D ** -0.5, 0.09375, ((1, 4),))
    conv_taps = centred(arg_keys[5], (3, CONV_CH), 3 ** -0.5, 3.5, ((1, 4),))
    proj_out = centred(arg_keys[6], (CONV_CH, D), CONV_CH ** -0.5, 0.1875, ((0, 4),))
    moe_in = centred(arg_keys[7], (TOKENS, D), 1.0, 6.0, ((0, 128),))
    moe_gain = jnp.clip(1.0 + 0.18 * jax.random.normal(arg_keys[8], (D,), jnp.float32), 0.1, 1.9)
    routes_keys = jax.random.split(jax.random.fold_in(arg_keys[9], 1), TOKENS // TOK_DEV)
    routes_turns = jax.random.permutation(jax.random.fold_in(arg_keys[9], 3), TOKENS // TOK_DEV)
    routes = jax.vmap(lambda own, number: assign_block(jax.random.fold_in(arg_keys[9], 2), own, number, TOK_DEV, EXPERTS, TOP, CAP, 2))(routes_keys, routes_turns).reshape((TOKENS, TOP))
    group_logits = centred(arg_keys[10], (TOKENS, GROUPS), 1.5, 6.0, ((0, 128),), jnp.float32)
    pair_logits = centred(arg_keys[11], (TOKENS, TOP), 1.5, 6.0, ((0, 128),), jnp.float32)
    expert_gate = centred(arg_keys[12], (EXPERTS, D, FF), D ** -0.5, 0.09375, ((0, 32), (2, 4)))
    expert_up = centred(arg_keys[13], (EXPERTS, D, FF), D ** -0.5, 0.09375, ((0, 32), (2, 4)))
    expert_down = centred(arg_keys[14], (EXPERTS, FF, D), FF ** -0.5, 0.125, ((0, 32), (1, 4)))
    return {"mix_in": mix_in, "mix_gain": mix_gain, "proj_b": proj_b, "proj_c": proj_c, "proj_h": proj_h, "conv_taps": conv_taps, "proj_out": proj_out, "moe_in": moe_in, "moe_gain": moe_gain, "routes": routes, "group_logits": group_logits, "pair_logits": pair_logits, "expert_gate": expert_gate, "expert_up": expert_up, "expert_down": expert_down}


def rms_scaled(values, gain_vec):
    widened = values.astype(jnp.float32)
    scaled = widened * lax.rsqrt(lax.optimization_barrier(jnp.mean(widened * widened, axis=-1, keepdims=True)) + 1e-06)
    return (scaled * gain_vec.astype(jnp.float32)).astype(jnp.bfloat16)

def reference(mix_in, mix_gain, proj_b, proj_c, proj_h, conv_taps, proj_out, moe_in, moe_gain, routes, group_logits, pair_logits, expert_gate, expert_up, expert_down):
    mix_norm = rms_scaled(mix_in, mix_gain)
    gate_b = jnp.dot(mix_norm, proj_b, preferred_element_type=jnp.float32).astype(jnp.bfloat16)
    gate_c = jnp.dot(mix_norm, proj_c, preferred_element_type=jnp.float32).astype(jnp.bfloat16)
    values_h = jnp.dot(mix_norm, proj_h, preferred_element_type=jnp.float32).astype(jnp.bfloat16)
    conv_in = gate_c.astype(jnp.float32) * values_h.astype(jnp.float32)
    padded = jnp.pad(conv_in, ((1, 1), (0, 0)))
    tap_vals = conv_taps.astype(jnp.float32)
    conv_out = tap_vals[0] * padded[:-2] + tap_vals[1] * padded[1:-1] + tap_vals[2] * padded[2:]
    mixed_rows = (gate_b.astype(jnp.float32) * conv_out).astype(jnp.bfloat16)
    ch_block = CONV_CH // N_TP
    mix_total = jnp.zeros((TOKENS, D), jnp.float32)
    for block_idx in range(N_TP):
        part_prod = jnp.dot(mixed_rows[:, block_idx * ch_block:(block_idx + 1) * ch_block], proj_out[block_idx * ch_block:(block_idx + 1) * ch_block], preferred_element_type=jnp.float32)
        mix_total = mix_total + lax.optimization_barrier(part_prod.astype(jnp.bfloat16)).astype(jnp.float32)
    moe_norm = rms_scaled(moe_in, moe_gain)
    sources = N_EP * N_TP
    route_pairs = routes.reshape(sources, TOP * TOK_DEV)
    route_hits = (route_pairs[:, :, None] == jnp.arange(EXPERTS, dtype=jnp.int32)[None, None, :]).astype(jnp.int32)
    route_ranks = lax.optimization_barrier(jnp.sum((jnp.cumsum(route_hits, axis=1) - route_hits) * route_hits, axis=2)).astype(jnp.int32)
    within = (jnp.arange(sources, dtype=jnp.int32)[:, None] * CAP + route_ranks).astype(jnp.int32)
    token_ids = (jnp.arange(sources, dtype=jnp.int32)[:, None] * TOK_DEV + jnp.arange(TOP * TOK_DEV, dtype=jnp.int32)[None, :] // TOP).astype(jnp.int32)
    group_prob = jax.nn.softmax(group_logits.astype(jnp.float32), axis=-1)
    member = routes // EXP_GROUP
    picked_prob = lax.optimization_barrier(jnp.sum(group_prob[:, None, :] * (member[:, :, None] == jnp.arange(GROUPS, dtype=jnp.int32)[None, None, :]).astype(jnp.float32), axis=-1))
    weight = picked_prob * jax.nn.softmax(pair_logits.astype(jnp.float32), axis=-1)
    index_table = jnp.full((EXPERTS, sources * CAP), TOKENS, jnp.int32).at[route_pairs.reshape(-1), within.reshape(-1)].set(token_ids.reshape(-1))
    weight_table = jnp.zeros((EXPERTS, sources * CAP), jnp.float32).at[route_pairs.reshape(-1), within.reshape(-1)].set(weight.reshape(-1))
    padded_norm = jnp.concatenate([moe_norm, jnp.zeros((1, D), jnp.bfloat16)], axis=0)
    ff_block = FF // N_TP

    def one_expert(run_total, inputs):
        index_row, weight_row, gate_mat, up_mat, down_mat = inputs
        row_data = padded_norm[index_row]
        gate_val = jnp.dot(row_data, gate_mat, preferred_element_type=jnp.float32)
        up_val = jnp.dot(row_data, up_mat, preferred_element_type=jnp.float32)
        hidden = (jax.nn.silu(gate_val) * up_val).astype(jnp.bfloat16)
        result = jnp.zeros((row_data.shape[0], D), jnp.float32)
        for block_idx in range(N_TP):
            down_part = jnp.dot(hidden[:, block_idx * ff_block:(block_idx + 1) * ff_block], down_mat[block_idx * ff_block:(block_idx + 1) * ff_block], preferred_element_type=jnp.float32)
            result = result + lax.optimization_barrier(down_part.astype(jnp.bfloat16)).astype(jnp.float32)
        rounded = lax.optimization_barrier(result.astype(jnp.bfloat16)).astype(jnp.float32)
        run_total = run_total.at[index_row].add(weight_row[:, None] * rounded, mode='drop')
        return (run_total, None)
    moe_total, _ = lax.scan(one_expert, jnp.zeros((TOKENS, D), jnp.float32), (index_table, weight_table, expert_gate, expert_up, expert_down))
    return (mix_total.astype(jnp.bfloat16), moe_total.astype(jnp.bfloat16))
```

```python
import jax
import jax.numpy as jnp
from jax import lax
from jax.experimental import pallas as pl
from jax.experimental.pallas import tpu as pltpu
from jax.sharding import PartitionSpec as P

GROUPS = 4
BF = jnp.bfloat16
F32 = jnp.float32
MESH = pl.DeviceIdType.MESH
SLOT = 16
NA = 18
NB = 14
NC = 4
PER = 3


def with_halo(cells, sides, width):
    for axis, dim in sides:
        count = lax.axis_size(axis)
        ends = count - 1
        head = lax.slice_in_dim(cells, 0, width, axis=dim)
        tail = lax.slice_in_dim(cells, cells.shape[dim] - width, cells.shape[dim], axis=dim)
        cells = jnp.concatenate(
            [
                lax.ppermute(tail, axis, [(i, (i + 1) % count) for i in range(ends)]),
                cells,
                lax.ppermute(head, axis, [((i + 1) % count, i) for i in range(ends)]),
            ],
            axis=dim,
        )
    return cells


def rms_scaled(values, gain_vec):
    widened = values.astype(F32)
    scaled = widened * lax.rsqrt(jnp.mean(widened * widened, axis=-1, keepdims=True) + 1e-06)
    return (scaled * gain_vec).astype(BF)


def tri(k):
    return (k * (k + 1)) // 2


def at_a(me, o, sign):
    z, y, c = me // 8, (me // 2) % 4, me % 2
    dz, dy, dc = tri(o // 6), tri((o // 2) % 3), o % 2
    return (((z + sign * dz + 4) % 4) * 4 + (y + sign * dy + 4) % 4) * 2 + (c + dc) % 2


def at_b(me, o, sign):
    z, y, c = me // 8, (me // 2) % 4, me % 2
    k = o // 2
    hi = k // 4
    dz = (1 - hi) * 2 + hi * tri(k - 4 * hi)
    dy = (1 - hi) * k + hi * 2
    return (((z + sign * dz + 4) % 4) * 4 + (y + sign * dy + 4) % 4) * 2 + (c + o % 2) % 2


def greet(me, x):
    barrier = pltpu.get_barrier_semaphore()

    def tell_a(o, _):
        pl.semaphore_signal(barrier, inc=1, device_id=(at_a(me, o, 1), x), device_id_type=MESH)
        return 0

    def tell_b(o, _):
        pl.semaphore_signal(barrier, inc=1, device_id=(at_b(me, o, 1), x), device_id_type=MESH)
        return 0

    lax.fori_loop(1, NA, tell_a, 0)
    lax.fori_loop(0, NB, tell_b, 0)
    pl.semaphore_signal(barrier, inc=1, device_id=(me, (x + 1) % 4), device_id_type=MESH)
    pl.semaphore_signal(barrier, inc=1, device_id=(me, (x + 3) % 4), device_id_type=MESH)
    pl.semaphore_wait(barrier, NA - 1 + NB + 2)


def remote(src, dst, send, recv, ep, tp):
    return pltpu.make_async_remote_copy(
        src_ref=src, dst_ref=dst, send_sem=send, recv_sem=recv, device_id=(ep, tp), device_id_type=MESH
    )


def slot_rows(base, rows, meta, hit0, hit1):
    want = lax.broadcasted_iota(jnp.int32, (rows, meta.shape[1]), 0) + base
    want = want.astype(F32)
    return jnp.where(meta[0:1] == want, hit0, 0.0) + jnp.where(meta[1:2] == want, hit1, 0.0)


def dispatch_kernel(
    norm, meta, gate_hbm, up_hbm,
    hid_a, hid_b, metas_out,
    tok, metas, oh_a, oh_b, out_a, out_b, recv_a, recv_b, gate_w, up_w, acc_g, acc_u, bcc_g, bcc_u,
    tok_s, tok_r, tokf_s, tokf_r, b_s, b_r, bx_s, bx_r, bf_s, bf_r, a_s, a_r, meta_s, meta_r, w_sem,
):
    me = lax.axis_index("ep")
    x = lax.axis_index("tp")
    right, left = (x + 1) % 4, (x + 3) % 4
    cw = tok.shape[3]
    rows = tok.shape[2]
    half = rows // 2
    hb = NB // 2
    gate_in = pltpu.make_async_copy(gate_hbm, gate_w, w_sem.at[0])
    up_in = pltpu.make_async_copy(up_hbm, up_w, w_sem.at[1])
    gate_in.start()
    up_in.start()
    greet(me, x)

    def cols(c):
        return pl.ds(pl.multiple_of(c * cw, cw), cw)

    meta_right = remote(meta, metas.at[1], meta_s.at[0], meta_r.at[0], me, right)
    meta_left = remote(meta, metas.at[2], meta_s.at[1], meta_r.at[1], me, left)
    meta_on = remote(metas.at[1], metas.at[3], meta_s.at[2], meta_r.at[2], me, right)
    meta_right.start()
    meta_left.start()

    def tok_right(c):
        return remote(norm.at[:, cols(c)], tok.at[c, 0], tok_s.at[c, 0], tok_r.at[c, 0], me, right)

    def tok_left(c):
        return remote(norm.at[:, cols(c)], tok.at[c, 1], tok_s.at[c, 1], tok_r.at[c, 1], me, left)

    def tok_on_right(c):
        return remote(tok.at[c, 0, pl.ds(0, half)], tok.at[c, 2, pl.ds(0, half)], tokf_s.at[c, 0], tokf_r.at[c, 0], me, right)

    def tok_on_left(c):
        return remote(tok.at[c, 1, pl.ds(half, half)], tok.at[c, 2, pl.ds(half, half)], tokf_s.at[c, 1], tokf_r.at[c, 1], me, left)

    def b_right(c):
        return remote(recv_b.at[c, 0], recv_b.at[c, 1], bx_s.at[c, 0], bx_r.at[c, 0], me, right)

    def b_left(c):
        return remote(recv_b.at[c, 0], recv_b.at[c, 2], bx_s.at[c, 1], bx_r.at[c, 1], me, left)

    def b_on_right(c):
        return remote(recv_b.at[c, 1, pl.ds(0, hb)], recv_b.at[c, 3, pl.ds(0, hb)], bf_s.at[c, 0], bf_r.at[c, 0], me, right)

    def b_on_left(c):
        return remote(recv_b.at[c, 2, pl.ds(hb, hb)], recv_b.at[c, 3, pl.ds(hb, hb)], bf_s.at[c, 1], bf_r.at[c, 1], me, left)

    def a_all(c):
        span = pl.ds(1, NA - 1)
        return remote(out_a.at[c, span], recv_a.at[c, span], a_s.at[c], a_r.at[c], me, right)

    def b_all(c):
        return remote(out_b.at[c], recv_b.at[c, 0], b_s.at[c], b_r.at[c], me, right)

    def first(c, _):
        tok_right(c).start()
        tok_left(c).start()
        return 0

    lax.fori_loop(0, NC, first, 0)

    own = meta[...]

    def hits_b(o, _):
        oh_b[o] = slot_rows(at_b(me, o, 1) * SLOT, SLOT, own, 1.0, 1.0).astype(BF)
        return 0

    lax.fori_loop(0, NB, hits_b, 0)

    def second(c, _):
        picked = jnp.dot(oh_b[...].reshape(NB * SLOT, rows), norm[:, cols(c)], preferred_element_type=F32)
        out_b[c] = picked.astype(BF).reshape(NB, SLOT, cw)

        def send(o, _):
            remote(out_b.at[c, o], recv_b.at[c, 0, o], b_s.at[c], b_r.at[c], at_b(me, o, 1), x).start()
            return 0

        lax.fori_loop(0, NB, send, 0)
        return 0

    lax.fori_loop(0, NC, second, 0)

    meta_right.wait()
    meta_on.start()
    meta_left.wait()
    meta_on.wait()
    metas[0] = own
    metas_out[...] = metas[...]

    def hits_a(o, _):
        base = at_a(me, o, 1) * SLOT
        for r in range(4):
            oh_a[r, o] = slot_rows(base, SLOT, metas_out[r], 1.0, 1.0).astype(BF)
        return 0

    lax.fori_loop(0, NA, hits_a, 0)

    def third(c, _):
        def pick(r, values):
            picked = jnp.dot(oh_a[r].reshape(NA * SLOT, rows), values, preferred_element_type=F32).astype(BF)
            picked = picked.reshape(NA, SLOT, cw)
            recv_a[c, 0, r] = picked[0]
            out_a[c, 1:, r] = picked[1:]

        pick(0, norm[:, cols(c)])
        tok_right(c).wait_recv()
        tok_on_right(c).start()
        tok_left(c).wait_recv()
        tok_on_left(c).start()
        pick(1, tok[c, 0])
        pick(2, tok[c, 1])
        tok_on_right(c).wait_recv()
        tok_on_left(c).wait_recv()
        pick(3, tok[c, 2])

        def send(o, _):
            remote(out_a.at[c, o], recv_a.at[c, o], a_s.at[c], a_r.at[c], at_a(me, o, 1), x).start()
            return 0

        lax.fori_loop(1, NA, send, 0)
        b_all(c).wait_recv()
        b_right(c).start()
        b_left(c).start()
        return 0

    lax.fori_loop(0, NC, third, 0)

    def fourth(c, _):
        b_right(c).wait_recv()
        b_on_right(c).start()
        b_left(c).wait_recv()
        b_on_left(c).start()
        return 0

    lax.fori_loop(0, NC, fourth, 0)
    gate_in.wait()
    up_in.wait()

    def finish(gate_val, up_val):
        return (gate_val / (1.0 + jnp.exp(-gate_val)) * up_val).astype(BF)

    for c in range(NC):
        a_all(c).wait_recv()

        def step_a(t, _, c=c):
            values = recv_a[c, pl.ds(t * PER, PER)].reshape(PER * 4 * SLOT, cw)
            g = jnp.dot(values, gate_w[c * cw:(c + 1) * cw], preferred_element_type=F32)
            u = jnp.dot(values, up_w[c * cw:(c + 1) * cw], preferred_element_type=F32)
            if c > 0:
                g = g + acc_g[t]
                u = u + acc_u[t]
            if c < NC - 1:
                acc_g[t] = g
                acc_u[t] = u
            else:
                hid_a[pl.ds(t * PER, PER)] = finish(g, u).reshape(PER, 4, SLOT, g.shape[1])
            return 0

        lax.fori_loop(0, NA // PER, step_a, 0)

    for c in range(NC):
        b_on_right(c).wait_recv()
        b_on_left(c).wait_recv()

        def step_b(r, _, c=c):
            values = recv_b[c, r].reshape(NB * SLOT, cw)
            g = jnp.dot(values, gate_w[c * cw:(c + 1) * cw], preferred_element_type=F32)
            u = jnp.dot(values, up_w[c * cw:(c + 1) * cw], preferred_element_type=F32)
            if c > 0:
                g = g + bcc_g[r]
                u = u + bcc_u[r]
            if c < NC - 1:
                bcc_g[r] = g
                bcc_u[r] = u
            else:
                hid_b[r] = finish(g, u).reshape(NB, SLOT, g.shape[1])
            return 0

        lax.fori_loop(0, 4, step_b, 0)

    def drain(c, _):
        tok_right(c).wait_send()
        tok_left(c).wait_send()
        tok_on_right(c).wait_send()
        tok_on_left(c).wait_send()
        b_all(c).wait_send()
        b_right(c).wait_send()
        b_left(c).wait_send()
        b_on_right(c).wait_send()
        b_on_left(c).wait_send()
        a_all(c).wait_send()
        return 0

    lax.fori_loop(0, NC, drain, 0)


def combine_kernel(
    hid_a, hid_b, metas, down_hbm,
    out,
    down_w, p_a, p_b, bh_in, bf_in, sum_b, ret_a, ret_b, w_a, w_b, p_t, th_in, tf_in, acc,
    bh_s, bh_r, bf_s, bf_r, b_s, b_r, a_s, a_r, th_s, th_r, tf_s, tf_r, w_sem,
):
    me = lax.axis_index("ep")
    x = lax.axis_index("tp")
    right, left = (x + 1) % 4, (x + 3) % 4
    cw = p_a.shape[4]
    rows = p_t.shape[2]
    half = rows // 2
    hb = NB // 2
    down_in = pltpu.make_async_copy(down_hbm, down_w, w_sem)
    down_in.start()
    greet(me, x)

    def cols(c):
        return pl.ds(pl.multiple_of(c * cw, cw), cw)

    def bh_right(c):
        return remote(p_b.at[c, 3, pl.ds(0, hb)], bh_in.at[c, 0], bh_s.at[c, 0], bh_r.at[c, 0], me, right)

    def bh_left(c):
        return remote(p_b.at[c, 3, pl.ds(hb, hb)], bh_in.at[c, 1], bh_s.at[c, 1], bh_r.at[c, 1], me, left)

    def bf_right(c):
        return remote(p_b.at[c, 2], bf_in.at[c, 0], bf_s.at[c, 0], bf_r.at[c, 0], me, right)

    def bf_left(c):
        return remote(p_b.at[c, 1], bf_in.at[c, 1], bf_s.at[c, 1], bf_r.at[c, 1], me, left)

    def th_right(c):
        return remote(p_t.at[c, 3, pl.ds(0, half)], th_in.at[c, 0], th_s.at[c, 0], th_r.at[c, 0], me, right)

    def th_left(c):
        return remote(p_t.at[c, 3, pl.ds(half, half)], th_in.at[c, 1], th_s.at[c, 1], th_r.at[c, 1], me, left)

    def tf_right(c):
        return remote(p_t.at[c, 2], tf_in.at[c, 0], tf_s.at[c, 0], tf_r.at[c, 0], me, right)

    def tf_left(c):
        return remote(p_t.at[c, 1], tf_in.at[c, 1], tf_s.at[c, 1], tf_r.at[c, 1], me, left)

    def a_all(c):
        span = pl.ds(1, NA - 1)
        return remote(p_a.at[c, span], ret_a.at[c, span], a_s.at[c], a_r.at[c], me, right)

    def b_all(c):
        return remote(sum_b.at[c], ret_b.at[c], b_s.at[c], b_r.at[c], me, right)

    down_in.wait()

    def first(c, _):
        def one(r, _):
            part = jnp.dot(hid_b[r].reshape(NB * SLOT, hid_b.shape[3]), down_w[:, cols(c)], preferred_element_type=F32)
            p_b[c, r] = part.astype(BF).reshape(NB, SLOT, cw)
            return 0

        lax.fori_loop(0, 4, one, 0)
        bh_right(c).start()
        bh_left(c).start()
        return 0

    lax.fori_loop(0, NC, first, 0)

    def second(c, _):
        def one(t, _):
            span = pl.ds(t * PER, PER)
            values = hid_a[span].reshape(PER * 4 * SLOT, hid_a.shape[3])
            part = jnp.dot(values, down_w[:, cols(c)], preferred_element_type=F32)
            p_a[c, span] = part.astype(BF).reshape(PER, 4, SLOT, cw)
            return 0

        lax.fori_loop(0, NA // PER, one, 0)

        def send(o, _):
            remote(p_a.at[c, o], ret_a.at[c, o], a_s.at[c], a_r.at[c], at_a(me, o, -1), x).start()
            return 0

        lax.fori_loop(1, NA, send, 0)
        ret_a[c, 0] = p_a[c, 0]
        bh_right(c).wait_recv()
        p_b[c, 2, :hb] = (p_b[c, 2, :hb].astype(F32) + bh_in[c, 0].astype(F32)).astype(BF)
        bf_right(c).start()
        bh_left(c).wait_recv()
        p_b[c, 1, hb:] = (p_b[c, 1, hb:].astype(F32) + bh_in[c, 1].astype(F32)).astype(BF)
        bf_left(c).start()
        return 0

    lax.fori_loop(0, NC, second, 0)

    def hits_a(o, _):
        base = at_a(me, o, 1) * SLOT
        for r in range(4):
            meta = metas[r]
            w_a[r, o] = slot_rows(base, SLOT, meta, meta[2:3], meta[3:4]).astype(BF)
        return 0

    lax.fori_loop(0, NA, hits_a, 0)

    def hits_b(o, _):
        meta = metas[0]
        w_b[o] = slot_rows(at_b(me, o, 1) * SLOT, SLOT, meta, meta[2:3], meta[3:4]).astype(BF)
        return 0

    lax.fori_loop(0, NB, hits_b, 0)

    def third(c, _):
        bf_right(c).wait_recv()
        bf_left(c).wait_recv()
        total = p_b[c, 0].astype(F32) + bf_in[c, 0].astype(F32) + bf_in[c, 1].astype(F32)
        sum_b[c] = total.astype(BF)

        def send(o, _):
            remote(sum_b.at[c, o], ret_b.at[c, o], b_s.at[c], b_r.at[c], at_b(me, o, -1), x).start()
            return 0

        lax.fori_loop(0, NB, send, 0)
        return 0

    lax.fori_loop(0, NC, third, 0)
    over_rows = (((0,), (0,)), ((), ()))

    def fourth(c, _):
        a_all(c).wait_recv()

        def weighed(r):
            values = ret_a[c, :, r].reshape(NA * SLOT, cw)
            return lax.dot_general(w_a[r].reshape(NA * SLOT, rows), values, over_rows, preferred_element_type=F32)

        p_t[c, 3] = weighed(3).astype(BF)
        th_right(c).start()
        th_left(c).start()
        p_t[c, 1] = weighed(1).astype(BF)
        p_t[c, 2] = weighed(2).astype(BF)
        acc[c] = weighed(0)
        th_right(c).wait_recv()
        p_t[c, 2, :half] = (p_t[c, 2, :half].astype(F32) + th_in[c, 0].astype(F32)).astype(BF)
        tf_right(c).start()
        th_left(c).wait_recv()
        p_t[c, 1, half:] = (p_t[c, 1, half:].astype(F32) + th_in[c, 1].astype(F32)).astype(BF)
        tf_left(c).start()
        return 0

    lax.fori_loop(0, NC, fourth, 0)

    def fifth(c, _):
        b_all(c).wait_recv()
        values = ret_b[c].reshape(NB * SLOT, cw)
        total = acc[c] + lax.dot_general(w_b[...].reshape(NB * SLOT, rows), values, over_rows, preferred_element_type=F32)
        tf_right(c).wait_recv()
        tf_left(c).wait_recv()
        total = total + tf_in[c, 0].astype(F32) + tf_in[c, 1].astype(F32)
        out[:, cols(c)] = total.astype(BF)
        return 0

    lax.fori_loop(0, NC, fifth, 0)

    def drain(c, _):
        bh_right(c).wait_send()
        bh_left(c).wait_send()
        bf_right(c).wait_send()
        bf_left(c).wait_send()
        th_right(c).wait_send()
        th_left(c).wait_send()
        tf_right(c).wait_send()
        tf_left(c).wait_send()
        a_all(c).wait_send()
        b_all(c).wait_send()
        return 0

    lax.fori_loop(0, NC, drain, 0)


VM = pltpu.VMEM
DMA = pltpu.SemaphoreType.DMA


def dispatch(norm, meta, gate_mat, up_mat):
    rows, width = norm.shape
    hidden = gate_mat.shape[1]
    cw = width // NC
    vmem = pl.BlockSpec(memory_space=VM)
    anywhere = pl.BlockSpec(memory_space=pl.ANY)
    return pl.pallas_call(
        dispatch_kernel,
        name="dispatch",
        out_shape=(
            jax.ShapeDtypeStruct((NA, 4, SLOT, hidden), BF),
            jax.ShapeDtypeStruct((4, NB, SLOT, hidden), BF),
            jax.ShapeDtypeStruct((4,) + meta.shape, F32),
        ),
        in_specs=[vmem, vmem, anywhere, anywhere],
        out_specs=(vmem, vmem, vmem),
        scratch_shapes=[
            VM((NC, 3, rows, cw), BF),
            VM((4,) + meta.shape, F32),
            VM((4, NA, SLOT, rows), BF),
            VM((NB, SLOT, rows), BF),
            VM((NC, NA, 4, SLOT, cw), BF),
            VM((NC, NB, SLOT, cw), BF),
            VM((NC, NA, 4, SLOT, cw), BF),
            VM((NC, 4, NB, SLOT, cw), BF),
            VM((width, hidden), BF),
            VM((width, hidden), BF),
            VM((NA // PER, PER * 4 * SLOT, hidden), F32),
            VM((NA // PER, PER * 4 * SLOT, hidden), F32),
            VM((4, NB * SLOT, hidden), F32),
            VM((4, NB * SLOT, hidden), F32),
            DMA((NC, 2)), DMA((NC, 2)), DMA((NC, 2)), DMA((NC, 2)),
            DMA((NC,)), DMA((NC,)),
            DMA((NC, 2)), DMA((NC, 2)), DMA((NC, 2)), DMA((NC, 2)),
            DMA((NC,)), DMA((NC,)),
            DMA((3,)), DMA((3,)), DMA((2,)),
        ],
        compiler_params=pltpu.CompilerParams(
            collective_id=0, has_side_effects=True, vmem_limit_bytes=64 * 1024 * 1024 - 65536
        ),
        cost_estimate=pl.CostEstimate(flops=100_000_000_000, bytes_accessed=12_000_000, transcendentals=0),
    )(norm, meta, gate_mat, up_mat)


def combine(hid_a, hid_b, metas, down_mat):
    rows = metas.shape[2]
    hidden, width = down_mat.shape
    cw = width // NC
    hb = NB // 2
    vmem = pl.BlockSpec(memory_space=VM)
    anywhere = pl.BlockSpec(memory_space=pl.ANY)
    return pl.pallas_call(
        combine_kernel,
        name="combine",
        out_shape=jax.ShapeDtypeStruct((rows, width), BF),
        in_specs=[vmem, vmem, vmem, anywhere],
        out_specs=vmem,
        scratch_shapes=[
            VM((hidden, width), BF),
            VM((NC, NA, 4, SLOT, cw), BF),
            VM((NC, 4, NB, SLOT, cw), BF),
            VM((NC, 2, hb, SLOT, cw), BF),
            VM((NC, 2, NB, SLOT, cw), BF),
            VM((NC, NB, SLOT, cw), BF),
            VM((NC, NA, 4, SLOT, cw), BF),
            VM((NC, NB, SLOT, cw), BF),
            VM((4, NA, SLOT, rows), BF),
            VM((NB, SLOT, rows), BF),
            VM((NC, 4, rows, cw), BF),
            VM((NC, 2, rows // 2, cw), BF),
            VM((NC, 2, rows, cw), BF),
            VM((NC, rows, cw), F32),
            DMA((NC, 2)), DMA((NC, 2)), DMA((NC, 2)), DMA((NC, 2)),
            DMA((NC,)), DMA((NC,)), DMA((NC,)), DMA((NC,)),
            DMA((NC, 2)), DMA((NC, 2)), DMA((NC, 2)), DMA((NC, 2)),
            DMA,
        ],
        compiler_params=pltpu.CompilerParams(
            collective_id=1, has_side_effects=True, vmem_limit_bytes=64 * 1024 * 1024 - 65536
        ),
        cost_estimate=pl.CostEstimate(flops=100_000_000_000, bytes_accessed=12_000_000, transcendentals=0),
    )(hid_a, hid_b, metas, down_mat)


def body(
    mix_in, mix_gain, proj_b, proj_c, proj_h, conv_taps, proj_out,
    moe_in, moe_gain, routes, group_logits, pair_logits, expert_gate, expert_up, expert_down,
):
    mix_norm = rms_scaled(mix_in, mix_gain)
    ch_width = proj_b.shape[1]
    row_piece = lax.all_gather(mix_norm, "tp", axis=0, tiled=True)

    moe_norm = rms_scaled(moe_in, moe_gain)
    local_rows, top_count = routes.shape
    experts_all = lax.axis_size("ep")
    flat_routes = routes.reshape(-1)
    route_hits = (flat_routes[:, None] == jnp.arange(experts_all, dtype=jnp.int32)[None, :]).astype(jnp.int32)
    route_ranks = jnp.sum((jnp.cumsum(route_hits, axis=0) - route_hits) * route_hits, axis=1)
    slot_ids = (flat_routes * SLOT + route_ranks).reshape(local_rows, top_count)
    group_prob = jax.nn.softmax(group_logits, axis=-1)
    member = routes // (experts_all // GROUPS)
    picked_prob = jnp.sum(
        group_prob[:, None, :]
        * (member[:, :, None] == jnp.arange(GROUPS, dtype=jnp.int32)[None, None, :]).astype(F32),
        axis=-1,
    )
    weight = picked_prob * jax.nn.softmax(pair_logits, axis=-1)
    meta = jnp.concatenate([slot_ids.astype(F32), weight, jnp.zeros((local_rows, 4), F32)], axis=1).T

    hid_a, hid_b, metas = dispatch(moe_norm, meta, expert_gate[0], expert_up[0])

    outputs = [
        jnp.dot(row_piece, weight_mat, preferred_element_type=F32).astype(BF)
        for weight_mat in (proj_b, proj_c, proj_h)
    ]
    projected = jnp.concatenate(outputs, axis=1)
    gate_b = projected[:, :ch_width]
    padded = with_halo(projected[:, ch_width:], (("ep", 0),), 1)
    conv_in = padded[:, :ch_width].astype(F32) * padded[:, ch_width:].astype(F32)
    tap_vals = conv_taps.astype(F32)
    conv_out = tap_vals[0] * conv_in[:-2] + tap_vals[1] * conv_in[1:-1] + tap_vals[2] * conv_in[2:]
    mixed_rows = (gate_b.astype(F32) * conv_out).astype(BF)
    mix_out = lax.psum_scatter(
        jnp.dot(mixed_rows, proj_out, preferred_element_type=F32).astype(BF),
        "tp",
        scatter_dimension=0,
        tiled=True,
    )
    moe_out = combine(hid_a, hid_b, metas, expert_down[0])
    return (mix_out, moe_out)


def solution(mesh):
    in_specs = (
        P(("ep", "tp"), None), P(), P(None, "tp"), P(None, "tp"), P(None, "tp"), P(None, "tp"), P("tp", None),
        P(("ep", "tp"), None), P(), P(("ep", "tp"), None), P(("ep", "tp"), None), P(("ep", "tp"), None),
        P("ep", None, "tp"), P("ep", None, "tp"), P("ep", "tp", None),
    )
    out_specs = (P(("ep", "tp"), None), P(("ep", "tp"), None))
    return jax.shard_map(body, mesh=mesh, in_specs=in_specs, out_specs=out_specs, check_vma=False)
```

```python
import jax
import jax.numpy as jnp
from jax import lax
from jax.experimental import pallas as pl
from jax.experimental.pallas import tpu as pltpu
from jax.sharding import PartitionSpec as P

GROUPS = 4
BF = jnp.bfloat16
F32 = jnp.float32
MESH = pl.DeviceIdType.MESH
SLOT = 16
NEAR = [(dz, dy, c) for dz, dy in ((0, 0), (1, 0), (3, 0), (0, 1), (0, 3), (1, 1), (3, 3), (1, 3), (3, 1)) for c in (0, 1)]
FAR = [(dz, dy, c) for dz, dy in ((2, 0), (0, 2), (2, 1), (2, 3), (1, 2), (3, 2), (2, 2)) for c in (0, 1)]
NA = len(NEAR)
NB = len(FAR)
NC = 4
PER = 3


def place(x, r):
    return (x + (3 * ((r * (r + 1)) // 2)) % 4) % 4


def peer(me, offset, sign):
    z, y, c = me // 8, (me // 2) % 4, me % 2
    dz, dy, dc = offset
    return (((z + sign * dz + 4) % 4) * 4 + (y + sign * dy + 4) % 4) * 2 + (c + dc) % 2


def greet(me, x):
    barrier = pltpu.get_barrier_semaphore()
    for offset in NEAR[1:] + FAR:
        pl.semaphore_signal(barrier, inc=1, device_id=(peer(me, offset, 1), x), device_id_type=MESH)
    pl.semaphore_signal(barrier, inc=1, device_id=(me, (x + 1) % 4), device_id_type=MESH)
    pl.semaphore_signal(barrier, inc=1, device_id=(me, (x + 3) % 4), device_id_type=MESH)
    pl.semaphore_wait(barrier, NA - 1 + NB + 2)


def remote(src, dst, send, recv, ep, tp):
    return pltpu.make_async_remote_copy(
        src_ref=src, dst_ref=dst, send_sem=send, recv_sem=recv, device_id=(ep, tp), device_id_type=MESH
    )


def slot_rows(base, rows, meta, hit0, hit1):
    want = lax.broadcasted_iota(jnp.int32, (rows, meta.shape[1]), 0) + base
    want = want.astype(F32)
    return jnp.where(meta[0:1] == want, hit0, 0.0) + jnp.where(meta[1:2] == want, hit1, 0.0)


def normed(raw, gain, into, width):
    step = 16
    cw = into.shape[3]

    def one(t, _):
        span = pl.ds(pl.multiple_of(t * step, step), step)
        values = raw[span, :].astype(F32)
        scale = lax.rsqrt(jnp.sum(values * values, axis=1, keepdims=True) * (1.0 / width) + 1e-06)
        values = (values * scale * gain[...]).astype(BF)
        for c in range(NC):
            into[c, 0, span, :] = values[:, c * cw:(c + 1) * cw]
        return 0

    lax.fori_loop(0, raw.shape[0] // step, one, 0)


def dispatch_kernel(
    moe_hbm, moe_gain, meta, gate_hbm, up_hbm, mix_hbm, mix_gain, projb_hbm, projc_hbm, projh_hbm, taps,
    hid_a, hid_b, metas_out, mixed,
    moe_raw, mix_raw, tok, mix, metas, oh_a, oh_b, out_a, out_b, recv_a, recv_b, gate_w, up_w, proj_w,
    bcc_g, bcc_u, cin, gate_b,
    tok_s, tok_r, tokf_s, tokf_r, mx_s, mx_r, mxf_s, mxf_r, b_s, b_r, bx_s, bx_r, bf_s, bf_r, a_s, a_r,
    meta_s, meta_r, halo_s, halo_r, w_sem,
):
    me = lax.axis_index("ep")
    x = lax.axis_index("tp")
    right, left = (x + 1) % 4, (x + 3) % 4
    rows, cw = tok.shape[2], tok.shape[3]
    width = NC * cw
    half = rows // 2
    hb = NB // 2
    chan = gate_b.shape[1]
    moe_in = pltpu.make_async_copy(moe_hbm, moe_raw, w_sem.at[0])
    mix_in = pltpu.make_async_copy(mix_hbm, mix_raw, w_sem.at[1])
    loads = [
        pltpu.make_async_copy(gate_hbm, gate_w, w_sem.at[2]),
        pltpu.make_async_copy(up_hbm, up_w, w_sem.at[3]),
        pltpu.make_async_copy(projb_hbm, proj_w.at[0], w_sem.at[4]),
        pltpu.make_async_copy(projc_hbm, proj_w.at[1], w_sem.at[5]),
        pltpu.make_async_copy(projh_hbm, proj_w.at[2], w_sem.at[6]),
    ]
    moe_in.start()
    mix_in.start()
    for load in loads:
        load.start()
    greet(me, x)

    meta_right = remote(meta, metas.at[1], meta_s.at[0], meta_r.at[0], me, right)
    meta_left = remote(meta, metas.at[2], meta_s.at[1], meta_r.at[1], me, left)
    meta_on = remote(metas.at[1], metas.at[3], meta_s.at[2], meta_r.at[2], me, right)
    meta_right.start()
    meta_left.start()

    def ring(buf, one_s, one_r, two_s, two_r):
        size = buf.shape[2] // 2
        lo, hi = pl.ds(0, size), pl.ds(size, size)
        return (
            lambda c: remote(buf.at[c, 0], buf.at[c, 1], one_s.at[c, 0], one_r.at[c, 0], me, right),
            lambda c: remote(buf.at[c, 0], buf.at[c, 2], one_s.at[c, 1], one_r.at[c, 1], me, left),
            lambda c: remote(buf.at[c, 1, lo], buf.at[c, 3, lo], two_s.at[c, 0], two_r.at[c, 0], me, right),
            lambda c: remote(buf.at[c, 2, hi], buf.at[c, 3, hi], two_s.at[c, 1], two_r.at[c, 1], me, left),
        )

    tok_right, tok_left, tok_on_right, tok_on_left = ring(tok, tok_s, tok_r, tokf_s, tokf_r)
    mix_right, mix_left, mix_on_right, mix_on_left = ring(mix, mx_s, mx_r, mxf_s, mxf_r)
    b_right, b_left, b_on_right, b_on_left = ring(recv_b, bx_s, bx_r, bf_s, bf_r)

    def a_all(c):
        span = pl.ds(1, NA - 1)
        return remote(out_a.at[c, span], recv_a.at[c, span], a_s.at[c], a_r.at[c], me, right)

    def b_all(c):
        return remote(out_b.at[c], recv_b.at[c, 0], b_s.at[c], b_r.at[c], me, right)

    moe_in.wait()
    normed(moe_raw, moe_gain, tok, width)

    def first(c, _):
        tok_right(c).start()
        tok_left(c).start()
        return 0

    lax.fori_loop(0, NC, first, 0)

    own = meta[...]
    for o in range(NB):
        oh_b[o] = slot_rows(peer(me, FAR[o], 1) * SLOT, SLOT, own, 1.0, 1.0).astype(BF)

    def second(c, _):
        picked = jnp.dot(oh_b[...].reshape(NB * SLOT, rows), tok[c, 0], preferred_element_type=F32)
        out_b[c] = picked.astype(BF).reshape(NB, SLOT, cw)
        for o in range(NB):
            remote(out_b.at[c, o], recv_b.at[c, 0, o], b_s.at[c], b_r.at[c], peer(me, FAR[o], 1), x).start()
        return 0

    lax.fori_loop(0, NC, second, 0)

    meta_right.wait()
    meta_on.start()
    meta_left.wait()
    meta_on.wait()
    metas[0] = own
    metas_out[...] = metas[...]
    for o in range(NA):
        base = peer(me, NEAR[o], 1) * SLOT
        for r in range(4):
            oh_a[r, o] = slot_rows(base, SLOT, metas_out[r], 1.0, 1.0).astype(BF)
    mix_in.wait()
    normed(mix_raw, mix_gain, mix, width)

    def third(c, _):
        def pick(r):
            picked = jnp.dot(oh_a[r].reshape(NA * SLOT, rows), tok[c, r], preferred_element_type=F32).astype(BF)
            picked = picked.reshape(NA, SLOT, cw)
            recv_a[c, 0, r] = picked[0]
            out_a[c, 1:, r] = picked[1:]

        pick(0)
        tok_right(c).wait_recv()
        tok_on_right(c).start()
        tok_left(c).wait_recv()
        tok_on_left(c).start()
        mix_right(c).start()
        mix_left(c).start()
        pick(1)
        pick(2)
        tok_on_right(c).wait_recv()
        tok_on_left(c).wait_recv()
        pick(3)
        for o in range(1, NA):
            remote(out_a.at[c, o], recv_a.at[c, o], a_s.at[c], a_r.at[c], peer(me, NEAR[o], 1), x).start()
        b_all(c).wait_recv()
        b_right(c).start()
        b_left(c).start()
        return 0

    lax.fori_loop(0, NC, third, 0)

    def fourth(c, _):
        mix_right(c).wait_recv()
        mix_on_right(c).start()
        mix_left(c).wait_recv()
        mix_on_left(c).start()
        b_right(c).wait_recv()
        b_on_right(c).start()
        b_left(c).wait_recv()
        b_on_left(c).start()
        return 0

    lax.fori_loop(0, NC, fourth, 0)
    for load in loads:
        load.wait()

    def finish(gate_val, up_val):
        return (gate_val / (1.0 + jnp.exp(-gate_val)) * up_val).astype(BF)

    def chunk_dots(values, mats, c):
        return [jnp.dot(values, mat[c * cw:(c + 1) * cw], preferred_element_type=F32) for mat in mats]

    for c in range(NC):
        a_all(c).wait_recv()

    def step_a(t, _):
        total = None
        for c in range(NC):
            values = recv_a[c, pl.ds(t * PER, PER)].reshape(PER * 4 * SLOT, cw)
            parts = chunk_dots(values, (gate_w, up_w), c)
            total = parts if total is None else [one + two for one, two in zip(total, parts)]
        hid_a[pl.ds(t * PER, PER)] = finish(*total).reshape(PER, 4, SLOT, gate_w.shape[1])
        return 0

    lax.fori_loop(0, NA // PER, step_a, 0)

    for c in range(NC):
        mix_on_right(c).wait_recv()
        mix_on_left(c).wait_recv()

    def project(r, _):
        start = pl.multiple_of(place(x, r) * rows, rows)
        total = None
        for c in range(NC):
            parts = chunk_dots(mix[c, r], [proj_w.at[n] for n in range(3)], c)
            total = parts if total is None else [one + two for one, two in zip(total, parts)]
        gate_b[pl.ds(start, rows)] = total[0].astype(BF)
        cin[pl.ds(start + 8, rows)] = total[1].astype(BF).astype(F32) * total[2].astype(BF).astype(F32)
        return 0

    lax.fori_loop(0, 4, project, 0)
    last = 4 * rows
    halo_next = remote(cin.at[pl.ds(last, 8)], cin.at[pl.ds(0, 8)], halo_s.at[0], halo_r.at[0], (me + 1) % 32, x)
    halo_prev = remote(cin.at[pl.ds(8, 8)], cin.at[pl.ds(last + 8, 8)], halo_s.at[1], halo_r.at[1], (me + 31) % 32, x)
    halo_next.start()
    halo_prev.start()

    for c in range(NC):
        b_on_right(c).wait_recv()
        b_on_left(c).wait_recv()

        def step_b(r, _, c=c):
            g, u = chunk_dots(recv_b[c, r].reshape(NB * SLOT, cw), (gate_w, up_w), c)
            if c > 0:
                g = g + bcc_g[r]
                u = u + bcc_u[r]
            if c < NC - 1:
                bcc_g[r] = g
                bcc_u[r] = u
            else:
                hid_b[r] = finish(g, u).reshape(NB, SLOT, g.shape[1])
            return 0

        lax.fori_loop(0, 4, step_b, 0)

    halo_next.wait()
    halo_prev.wait()
    cin[0:8] = cin[0:8] * jnp.where(me > 0, 1.0, 0.0)
    cin[last + 8:last + 16] = cin[last + 8:last + 16] * jnp.where(me < 31, 1.0, 0.0)
    tap = taps[...].astype(F32)
    conv = tap[0:1] * cin[7:last + 7] + tap[1:2] * cin[8:last + 8] + tap[2:3] * cin[9:last + 9]
    mixed[...] = (gate_b[...].astype(F32) * conv).astype(BF)

    def drain(c, _):
        for copy in (
            tok_right, tok_left, tok_on_right, tok_on_left, mix_right, mix_left, mix_on_right, mix_on_left,
            b_all, b_right, b_left, b_on_right, b_on_left, a_all,
        ):
            copy(c).wait_send()
        return 0

    lax.fori_loop(0, NC, drain, 0)


def combine_kernel(
    hid_a, hid_b, metas, down_hbm, mixed, proj_hbm,
    out, mix_out,
    down_w, proj_w, p_a, p_b, bh_in, bf_in, sum_b, ret_a, ret_b, w_a, w_b, p_t, th_in, tf_in, p_m, mh_in, mf_in,
    bh_s, bh_r, bf_s, bf_r, b_s, b_r, a_s, a_r, th_s, th_r, tf_s, tf_r, mh_s, mh_r, mf_s, mf_r, w_sem,
):
    me = lax.axis_index("ep")
    x = lax.axis_index("tp")
    right, left = (x + 1) % 4, (x + 3) % 4
    cw = p_a.shape[4]
    rows = p_t.shape[2]
    half = rows // 2
    hb = NB // 2
    down_in = pltpu.make_async_copy(down_hbm, down_w, w_sem.at[0])
    proj_in = pltpu.make_async_copy(proj_hbm, proj_w, w_sem.at[1])
    down_in.start()
    proj_in.start()
    greet(me, x)

    def cols(c):
        return pl.ds(pl.multiple_of(c * cw, cw), cw)

    def ring(buf, halves, wholes, one_s, one_r, two_s, two_r):
        size = buf.shape[2] // 2
        top = buf.shape[1] - 1
        return (
            lambda c: remote(buf.at[c, top, pl.ds(0, size)], halves.at[c, 0], one_s.at[c, 0], one_r.at[c, 0], me, right),
            lambda c: remote(buf.at[c, top, pl.ds(size, size)], halves.at[c, 1], one_s.at[c, 1], one_r.at[c, 1], me, left),
            lambda c: remote(buf.at[c, top - 1], wholes.at[c, 0], two_s.at[c, 0], two_r.at[c, 0], me, right),
            lambda c: remote(buf.at[c, top - 2], wholes.at[c, 1], two_s.at[c, 1], two_r.at[c, 1], me, left),
        )

    b_ring = ring(p_b, bh_in, bf_in, bh_s, bh_r, bf_s, bf_r)
    t_ring = ring(p_t, th_in, tf_in, th_s, th_r, tf_s, tf_r)
    m_ring = ring(p_m, mh_in, mf_in, mh_s, mh_r, mf_s, mf_r)

    def open_ring(copies, c):
        copies[0](c).start()
        copies[1](c).start()

    def pass_on(copies, buf, halves, c):
        size = buf.shape[2] // 2
        top = buf.shape[1] - 1
        copies[0](c).wait_recv()
        buf[c, top - 1, :size] = (buf[c, top - 1, :size].astype(F32) + halves[c, 0].astype(F32)).astype(BF)
        copies[2](c).start()
        copies[1](c).wait_recv()
        buf[c, top - 2, size:] = (buf[c, top - 2, size:].astype(F32) + halves[c, 1].astype(F32)).astype(BF)
        copies[3](c).start()

    def arrivals(copies, wholes, c):
        copies[2](c).wait_recv()
        copies[3](c).wait_recv()
        return wholes[c, 0].astype(F32) + wholes[c, 1].astype(F32)

    def a_all(c):
        span = pl.ds(1, NA - 1)
        return remote(p_a.at[c, span], ret_a.at[c, span], a_s.at[c], a_r.at[c], me, right)

    def b_all(c):
        return remote(sum_b.at[c], ret_b.at[c], b_s.at[c], b_r.at[c], me, right)

    down_in.wait()

    def first(c, _):
        def one(r, _):
            part = jnp.dot(hid_b[r].reshape(NB * SLOT, hid_b.shape[3]), down_w[:, cols(c)], preferred_element_type=F32)
            p_b[c, r] = part.astype(BF).reshape(NB, SLOT, cw)
            return 0

        lax.fori_loop(0, 4, one, 0)
        open_ring(b_ring, c)
        return 0

    lax.fori_loop(0, NC, first, 0)

    def second(c, _):
        def one(t, _):
            span = pl.ds(t * PER, PER)
            values = hid_a[span].reshape(PER * 4 * SLOT, hid_a.shape[3])
            part = jnp.dot(values, down_w[:, cols(c)], preferred_element_type=F32)
            p_a[c, span] = part.astype(BF).reshape(PER, 4, SLOT, cw)
            return 0

        lax.fori_loop(0, NA // PER, one, 0)
        for o in range(1, NA):
            remote(p_a.at[c, o], ret_a.at[c, o], a_s.at[c], a_r.at[c], peer(me, NEAR[o], -1), x).start()
        ret_a[c, 0] = p_a[c, 0]
        pass_on(b_ring, p_b, bh_in, c)
        return 0

    lax.fori_loop(0, NC, second, 0)
    proj_in.wait()

    def mixer(c, _):
        def one(r, _):
            values = mixed[pl.ds(pl.multiple_of(place(x, r) * rows, rows), rows)]
            p_m[c, r] = jnp.dot(values, proj_w[:, cols(c)], preferred_element_type=F32).astype(BF)
            return 0

        lax.fori_loop(0, 4, one, 0)
        open_ring(m_ring, c)
        return 0

    lax.fori_loop(0, NC, mixer, 0)

    for o in range(NA):
        base = peer(me, NEAR[o], 1) * SLOT
        for r in range(4):
            meta = metas[r]
            w_a[r, o] = slot_rows(base, SLOT, meta, meta[2:3], meta[3:4]).astype(BF)
    for o in range(NB):
        meta = metas[0]
        w_b[o] = slot_rows(peer(me, FAR[o], 1) * SLOT, SLOT, meta, meta[2:3], meta[3:4]).astype(BF)

    def third(c, _):
        sum_b[c] = (p_b[c, 0].astype(F32) + arrivals(b_ring, bf_in, c)).astype(BF)
        for o in range(NB):
            remote(sum_b.at[c, o], ret_b.at[c, o], b_s.at[c], b_r.at[c], peer(me, FAR[o], -1), x).start()
        pass_on(m_ring, p_m, mh_in, c)
        return 0

    lax.fori_loop(0, NC, third, 0)
    over_rows = (((0,), (0,)), ((), ()))

    def weighed(r, c):
        values = ret_a[c, :, r].reshape(NA * SLOT, cw)
        return lax.dot_general(w_a[r].reshape(NA * SLOT, rows), values, over_rows, preferred_element_type=F32)

    def fourth(c, _):
        a_all(c).wait_recv()
        p_t[c, 2] = weighed(3, c).astype(BF)
        open_ring(t_ring, c)
        p_t[c, 0] = weighed(1, c).astype(BF)
        p_t[c, 1] = weighed(2, c).astype(BF)
        pass_on(t_ring, p_t, th_in, c)
        return 0

    lax.fori_loop(0, NC, fourth, 0)

    def fifth(c, _):
        mix_out[:, cols(c)] = (p_m[c, 0].astype(F32) + arrivals(m_ring, mf_in, c)).astype(BF)
        return 0

    lax.fori_loop(0, NC, fifth, 0)

    def sixth(c, _):
        b_all(c).wait_recv()
        values = ret_b[c].reshape(NB * SLOT, cw)
        total = weighed(0, c) + lax.dot_general(
            w_b[...].reshape(NB * SLOT, rows), values, over_rows, preferred_element_type=F32
        )
        out[:, cols(c)] = (total + arrivals(t_ring, tf_in, c)).astype(BF)
        return 0

    lax.fori_loop(0, NC, sixth, 0)

    def drain(c, _):
        for copy in b_ring + t_ring + m_ring + (a_all, b_all):
            copy(c).wait_send()
        return 0

    lax.fori_loop(0, NC, drain, 0)


VM = pltpu.VMEM
DMA = pltpu.SemaphoreType.DMA
PARAMS = dict(has_side_effects=True, vmem_limit_bytes=64 * 1024 * 1024 - 65536)
COST = pl.CostEstimate(flops=100_000_000_000, bytes_accessed=12_000_000, transcendentals=0)


def specs(places):
    vmem = pl.BlockSpec(memory_space=VM)
    anywhere = pl.BlockSpec(memory_space=pl.ANY)
    return [vmem if place == "v" else anywhere for place in places]


def dispatch(moe_in, moe_gain, meta, gate_mat, up_mat, mix_in, mix_gain, proj_b, proj_c, proj_h, taps):
    rows, width = moe_in.shape
    hidden = gate_mat.shape[1]
    chan = proj_b.shape[1]
    cw = width // NC
    pair = DMA((NC, 2))
    single = DMA((NC,))
    return pl.pallas_call(
        dispatch_kernel,
        name="dispatch",
        out_shape=(
            jax.ShapeDtypeStruct((NA, 4, SLOT, hidden), BF),
            jax.ShapeDtypeStruct((4, NB, SLOT, hidden), BF),
            jax.ShapeDtypeStruct((4,) + meta.shape, F32),
            jax.ShapeDtypeStruct((4 * rows, chan), BF),
        ),
        in_specs=specs("avvaaavaaav"),
        out_specs=tuple(specs("vvvv")),
        scratch_shapes=[
            VM((rows, width), BF),
            VM((rows, width), BF),
            VM((NC, 4, rows, cw), BF),
            VM((NC, 4, rows, cw), BF),
            VM((4,) + meta.shape, F32),
            VM((4, NA, SLOT, rows), BF),
            VM((NB, SLOT, rows), BF),
            VM((NC, NA, 4, SLOT, cw), BF),
            VM((NC, NB, SLOT, cw), BF),
            VM((NC, NA, 4, SLOT, cw), BF),
            VM((NC, 4, NB, SLOT, cw), BF),
            VM((width, hidden), BF),
            VM((width, hidden), BF),
            VM((3, width, chan), BF),
            VM((4, NB * SLOT, hidden), F32),
            VM((4, NB * SLOT, hidden), F32),
            VM((4 * rows + 16, chan), F32),
            VM((4 * rows, chan), BF),
            pair, pair, pair, pair, pair, pair, pair, pair, single, single, pair, pair, pair, pair, single, single,
            DMA((3,)), DMA((3,)), DMA((2,)), DMA((2,)), DMA((7,)),
        ],
        compiler_params=pltpu.CompilerParams(collective_id=0, **PARAMS),
        cost_estimate=COST,
    )(moe_in, moe_gain, meta, gate_mat, up_mat, mix_in, mix_gain, proj_b, proj_c, proj_h, taps)


def combine(hid_a, hid_b, metas, down_mat, mixed, proj_out):
    rows = metas.shape[2]
    hidden, width = down_mat.shape
    chan = proj_out.shape[0]
    cw = width // NC
    hb = NB // 2
    pair = DMA((NC, 2))
    single = DMA((NC,))
    return pl.pallas_call(
        combine_kernel,
        name="combine",
        out_shape=(jax.ShapeDtypeStruct((rows, width), BF), jax.ShapeDtypeStruct((rows, width), BF)),
        in_specs=specs("vvvava"),
        out_specs=tuple(specs("vv")),
        scratch_shapes=[
            VM((hidden, width), BF),
            VM((chan, width), BF),
            VM((NC, NA, 4, SLOT, cw), BF),
            VM((NC, 4, NB, SLOT, cw), BF),
            VM((NC, 2, hb, SLOT, cw), BF),
            VM((NC, 2, NB, SLOT, cw), BF),
            VM((NC, NB, SLOT, cw), BF),
            VM((NC, NA, 4, SLOT, cw), BF),
            VM((NC, NB, SLOT, cw), BF),
            VM((4, NA, SLOT, rows), BF),
            VM((NB, SLOT, rows), BF),
            VM((NC, 3, rows, cw), BF),
            VM((NC, 2, rows // 2, cw), BF),
            VM((NC, 2, rows, cw), BF),
            VM((NC, 4, rows, cw), BF),
            VM((NC, 2, rows // 2, cw), BF),
            VM((NC, 2, rows, cw), BF),
            pair, pair, pair, pair, single, single, single, single,
            pair, pair, pair, pair, pair, pair, pair, pair, DMA((2,)),
        ],
        compiler_params=pltpu.CompilerParams(collective_id=1, **PARAMS),
        cost_estimate=COST,
    )(hid_a, hid_b, metas, down_mat, mixed, proj_out)


def body(
    mix_in, mix_gain, proj_b, proj_c, proj_h, conv_taps, proj_out,
    moe_in, moe_gain, routes, group_logits, pair_logits, expert_gate, expert_up, expert_down,
):
    local_rows, top_count = routes.shape
    experts_all = lax.axis_size("ep")
    flat_routes = routes.reshape(-1)
    route_hits = (flat_routes[:, None] == jnp.arange(experts_all, dtype=jnp.int32)[None, :]).astype(jnp.int32)
    route_ranks = jnp.sum((jnp.cumsum(route_hits, axis=0) - route_hits) * route_hits, axis=1)
    slot_ids = (flat_routes * SLOT + route_ranks).reshape(local_rows, top_count)
    group_prob = jax.nn.softmax(group_logits, axis=-1)
    member = routes // (experts_all // GROUPS)
    picked_prob = jnp.sum(
        group_prob[:, None, :]
        * (member[:, :, None] == jnp.arange(GROUPS, dtype=jnp.int32)[None, None, :]).astype(F32),
        axis=-1,
    )
    weight = picked_prob * jax.nn.softmax(pair_logits, axis=-1)
    meta = jnp.concatenate([slot_ids.astype(F32), weight, jnp.zeros((local_rows, 4), F32)], axis=1).T

    hid_a, hid_b, metas, mixed = dispatch(
        moe_in, moe_gain[None, :], meta, expert_gate[0], expert_up[0],
        mix_in, mix_gain[None, :], proj_b, proj_c, proj_h, conv_taps,
    )
    moe_out, mix_out = combine(hid_a, hid_b, metas, expert_down[0], mixed, proj_out)
    return (mix_out, moe_out)


def solution(mesh):
    in_specs = (
        P(("ep", "tp"), None), P(), P(None, "tp"), P(None, "tp"), P(None, "tp"), P(None, "tp"), P("tp", None),
        P(("ep", "tp"), None), P(), P(("ep", "tp"), None), P(("ep", "tp"), None), P(("ep", "tp"), None),
        P("ep", None, "tp"), P("ep", None, "tp"), P("ep", "tp", None),
    )
    out_specs = (P(("ep", "tp"), None), P(("ep", "tp"), None))
    return jax.shard_map(body, mesh=mesh, in_specs=in_specs, out_specs=out_specs, check_vma=False)
```

```python
import jax
import jax.numpy as jnp
from jax import lax
from jax.experimental import pallas as pl
from jax.experimental.pallas import tpu as pltpu
from jax.sharding import PartitionSpec as P

GROUPS = 4
BF = jnp.bfloat16
F32 = jnp.float32
MESH = pl.DeviceIdType.MESH
SLOT = 16
def both(*chips):
    return [(dz, dy, c) for dz, dy in chips for c in (0, 1)]


NEAR = both((0, 0), (1, 0), (3, 0), (0, 1), (0, 3)) + [(2, 0, 0), (0, 2, 0)] + both((1, 1), (3, 3), (1, 3), (3, 1))
FAR = [(2, 0, 1), (0, 2, 1)] + both((2, 1), (2, 3), (1, 2), (3, 2), (2, 2))
NA = len(NEAR)
NB = len(FAR)
NC = 4
PER = 4


def place(x, r):
    return (x + (3 * ((r * (r + 1)) // 2)) % 4) % 4


def peer(me, offset, sign):
    z, y, c = me // 8, (me // 2) % 4, me % 2
    dz, dy, dc = offset
    return (((z + sign * dz + 4) % 4) * 4 + (y + sign * dy + 4) % 4) * 2 + (c + dc) % 2


def greet(me, x):
    barrier = pltpu.get_barrier_semaphore()
    for offset in NEAR[1:] + FAR:
        pl.semaphore_signal(barrier, inc=1, device_id=(peer(me, offset, 1), x), device_id_type=MESH)
    pl.semaphore_signal(barrier, inc=1, device_id=(me, (x + 1) % 4), device_id_type=MESH)
    pl.semaphore_signal(barrier, inc=1, device_id=(me, (x + 3) % 4), device_id_type=MESH)
    return lambda: pl.semaphore_wait(barrier, NA - 1 + NB + 2)


def remote(src, dst, send, recv, ep, tp):
    return pltpu.make_async_remote_copy(
        src_ref=src, dst_ref=dst, send_sem=send, recv_sem=recv, device_id=(ep, tp), device_id_type=MESH
    )


def slot_rows(base, rows, meta, hit0, hit1):
    want = lax.broadcasted_iota(jnp.int32, (rows, meta.shape[1]), 0) + base
    want = want.astype(F32)
    return jnp.where(meta[0:1] == want, hit0, 0.0) + jnp.where(meta[1:2] == want, hit1, 0.0)


def routing(routes, group_logits, pair_logits):
    count = routes.shape[1]
    r0, r1 = routes[0:1], routes[1:2]
    expert = lax.broadcasted_iota(jnp.int32, (32, count), 0)
    hit0, hit1 = jnp.where(expert == r0, 1.0, 0.0), jnp.where(expert == r1, 1.0, 0.0)
    earlier = lax.broadcasted_iota(jnp.int32, (count, count), 0) < lax.broadcasted_iota(jnp.int32, (count, count), 1)
    before = jnp.dot((hit0 + hit1).astype(BF), jnp.where(earlier, 1.0, 0.0).astype(BF), preferred_element_type=F32)

    def share(logits):
        grown = jnp.exp(logits - jnp.max(logits, axis=0, keepdims=True))
        return grown / jnp.sum(grown, axis=0, keepdims=True)

    group, pair = share(group_logits), share(pair_logits)

    def one(route, hit, k):
        slot = route.astype(F32) * SLOT + jnp.sum(before * hit, axis=0, keepdims=True)
        member = sum(
            group[g:g + 1] * jnp.where(jnp.logical_and(route >= 8 * g, route < 8 * g + 8), 1.0, 0.0) for g in range(GROUPS)
        )
        return slot, member * pair[k:k + 1]

    slot0, weight0 = one(r0, hit0, 0)
    slot1, weight1 = one(r1, hit1, 1)
    return jnp.concatenate([slot0, slot1, weight0, weight1, jnp.zeros((4, count), F32)], axis=0)


def normed(raw, gain, into, width):
    step = 16
    cw = into.shape[3]

    def one(t, _):
        span = pl.ds(pl.multiple_of(t * step, step), step)
        values = raw[span, :].astype(F32)
        scale = lax.rsqrt(jnp.sum(values * values, axis=1, keepdims=True) * (1.0 / width) + 1e-06)
        values = (values * scale * gain[...]).astype(BF)
        for c in range(NC):
            into[c, 0, span, :] = values[:, c * cw:(c + 1) * cw]
        return 0

    lax.fori_loop(0, raw.shape[0] // step, one, 0)


def dispatch_kernel(
    moe_hbm, moe_gain, routes, group_logits, pair_logits, gate_hbm, up_hbm, mix_hbm, mix_gain, projb_hbm, projc_hbm, projh_hbm, taps,
    hid_a, hid_b, metas_out, mixed,
    raw, tok, mix, metas, oh_a, oh_b, out_a, out_b, recv_a, recv_b, gate_w, up_w, proj_w,
    acc_g, acc_u, bcc_g, bcc_u, cin, gate_b,
    tok_s, tok_r, tokf_s, tokf_r, mx_s, mx_r, mxf_s, mxf_r, b_s, b_r, bx_s, bx_r, bf_s, bf_r, a_s, a_r,
    meta_s, meta_r, halo_s, halo_r, w_sem,
):
    me = lax.axis_index("ep")
    x = lax.axis_index("tp")
    right, left = (x + 1) % 4, (x + 3) % 4
    rows, cw = tok.shape[2], tok.shape[3]
    width = NC * cw
    half = rows // 2
    hb = NB // 2
    chan = gate_b.shape[1]
    moe_in = pltpu.make_async_copy(moe_hbm, raw, w_sem.at[0])
    mix_in = pltpu.make_async_copy(mix_hbm, raw, w_sem.at[1])
    loads = [
        pltpu.make_async_copy(gate_hbm, gate_w, w_sem.at[2]),
        pltpu.make_async_copy(up_hbm, up_w, w_sem.at[3]),
        pltpu.make_async_copy(projb_hbm, proj_w.at[0], w_sem.at[4]),
        pltpu.make_async_copy(projc_hbm, proj_w.at[1], w_sem.at[5]),
        pltpu.make_async_copy(projh_hbm, proj_w.at[2], w_sem.at[6]),
    ]
    moe_in.start()
    everyone_in = greet(me, x)
    for load in loads:
        load.start()
    metas[0] = routing(routes[...], group_logits[...], pair_logits[...])
    moe_in.wait()
    normed(raw, moe_gain, tok, width)
    mix_in.start()
    everyone_in()

    meta_right = remote(metas.at[0], metas.at[1], meta_s.at[0], meta_r.at[0], me, right)
    meta_left = remote(metas.at[0], metas.at[2], meta_s.at[1], meta_r.at[1], me, left)
    meta_on = remote(metas.at[1], metas.at[3], meta_s.at[2], meta_r.at[2], me, right)
    meta_right.start()
    meta_left.start()

    def ring(buf, one_s, one_r, two_s, two_r):
        size = buf.shape[2] // 2
        lo, hi = pl.ds(0, size), pl.ds(size, size)
        return (
            lambda c: remote(buf.at[c, 0], buf.at[c, 1], one_s.at[c, 0], one_r.at[c, 0], me, right),
            lambda c: remote(buf.at[c, 0], buf.at[c, 2], one_s.at[c, 1], one_r.at[c, 1], me, left),
            lambda c: remote(buf.at[c, 1, lo], buf.at[c, 3, lo], two_s.at[c, 0], two_r.at[c, 0], me, right),
            lambda c: remote(buf.at[c, 2, hi], buf.at[c, 3, hi], two_s.at[c, 1], two_r.at[c, 1], me, left),
        )

    tok_right, tok_left, tok_on_right, tok_on_left = ring(tok, tok_s, tok_r, tokf_s, tokf_r)
    mix_right, mix_left, mix_on_right, mix_on_left = ring(mix, mx_s, mx_r, mxf_s, mxf_r)
    b_right, b_left, b_on_right, b_on_left = ring(recv_b, bx_s, bx_r, bf_s, bf_r)

    def a_all(c):
        span = pl.ds(1, NA - 1)
        return remote(out_a.at[c, span], recv_a.at[c, span], a_s.at[c], a_r.at[c], me, right)

    def b_all(c):
        return remote(out_b.at[c], recv_b.at[c, 0], b_s.at[c], b_r.at[c], me, right)

    def first(c, _):
        tok_right(c).start()
        tok_left(c).start()
        return 0

    lax.fori_loop(0, NC, first, 0)

    own = metas[0]
    for o in range(NB):
        oh_b[o] = slot_rows(peer(me, FAR[o], 1) * SLOT, SLOT, own, 1.0, 1.0).astype(BF)

    def second(c, _):
        picked = jnp.dot(oh_b[...].reshape(NB * SLOT, rows), tok[c, 0], preferred_element_type=F32)
        out_b[c] = picked.astype(BF).reshape(NB, SLOT, cw)
        for o in range(NB):
            remote(out_b.at[c, o], recv_b.at[c, 0, o], b_s.at[c], b_r.at[c], peer(me, FAR[o], 1), x).start()
        return 0

    lax.fori_loop(0, NC, second, 0)

    meta_right.wait()
    meta_on.start()
    meta_left.wait()
    meta_on.wait()
    metas_out[...] = metas[...]
    for o in range(NA):
        base = peer(me, NEAR[o], 1) * SLOT
        for r in range(4):
            oh_a[r, o] = slot_rows(base, SLOT, metas_out[r], 1.0, 1.0).astype(BF)
    mix_in.wait()
    normed(raw, mix_gain, mix, width)

    def pick(c, r):
        picked = jnp.dot(oh_a[r].reshape(NA * SLOT, rows), tok[c, r], preferred_element_type=F32).astype(BF)
        picked = picked.reshape(NA, SLOT, cw)
        recv_a[c, 0, r] = picked[0]
        out_a[c, 1:, r] = picked[1:]

    def third(c, _):
        tok_right(c).wait_recv()
        tok_on_right(c).start()
        tok_left(c).wait_recv()
        tok_on_left(c).start()
        pick(c, 0)
        pick(c, 1)
        pick(c, 2)
        return 0

    lax.fori_loop(0, NC, third, 0)

    def mix_first(c, _):
        mix_right(c).start()
        mix_left(c).start()
        return 0

    lax.fori_loop(0, NC, mix_first, 0)

    def fourth(c, _):
        tok_on_right(c).wait_recv()
        tok_on_left(c).wait_recv()
        pick(c, 3)
        for o in range(1, NA):
            remote(out_a.at[c, o], recv_a.at[c, o], a_s.at[c], a_r.at[c], peer(me, NEAR[o], 1), x).start()
        return 0

    lax.fori_loop(0, NC, fourth, 0)

    def b_first(c, _):
        b_all(c).wait_recv()
        b_right(c).start()
        b_left(c).start()
        return 0

    lax.fori_loop(0, NC, b_first, 0)

    def mix_second(c, _):
        mix_right(c).wait_recv()
        mix_on_right(c).start()
        mix_left(c).wait_recv()
        mix_on_left(c).start()
        return 0

    lax.fori_loop(0, NC, mix_second, 0)

    def b_second(c):
        b_right(c).wait_recv()
        b_on_right(c).start()
        b_left(c).wait_recv()
        b_on_left(c).start()

    for load in loads:
        load.wait()

    def finish(gate_val, up_val):
        return (gate_val / (1.0 + jnp.exp(-gate_val)) * up_val).astype(BF)

    def chunk_dots(values, mats, c):
        return [jnp.dot(values, mat[c * cw:(c + 1) * cw], preferred_element_type=F32) for mat in mats]

    def steps(c, count, rows_of, sums, store):
        def step(t, _):
            g, u = chunk_dots(rows_of(t), (gate_w, up_w), c)
            if c > 0:
                g = g + sums[0][t]
                u = u + sums[1][t]
            if c < NC - 1:
                sums[0][t] = g
                sums[1][t] = u
            else:
                store(t, finish(g, u))
            return 0

        lax.fori_loop(0, count, step, 0)

    def store_a(t, values):
        hid_a[pl.ds(t * PER, PER)] = values.reshape(PER, 4, SLOT, gate_w.shape[1])

    def store_b(r, values):
        hid_b[r] = values.reshape(NB, SLOT, gate_w.shape[1])

    def a_steps(c):
        a_all(c).wait_recv()
        steps(
            c, NA // PER, lambda t: recv_a[c, pl.ds(t * PER, PER)].reshape(PER * 4 * SLOT, cw), (acc_g, acc_u), store_a
        )

    def b_steps(c):
        b_on_right(c).wait_recv()
        b_on_left(c).wait_recv()
        steps(c, 4, lambda r: recv_b[c, r].reshape(NB * SLOT, cw), (bcc_g, bcc_u), store_b)

    a_steps(0)
    b_second(0)
    a_steps(1)
    b_second(1)
    b_second(2)
    a_steps(2)
    b_second(3)

    for c in range(NC):
        mix_on_right(c).wait_recv()
        mix_on_left(c).wait_recv()

    def project(r, _):
        start = pl.multiple_of(place(x, r) * rows, rows)
        total = None
        for c in range(NC):
            parts = chunk_dots(mix[c, r], [proj_w.at[n] for n in range(3)], c)
            total = parts if total is None else [one + two for one, two in zip(total, parts)]
        gate_b[pl.ds(start, rows)] = total[0].astype(BF)
        cin[pl.ds(start + 8, rows)] = total[1].astype(BF).astype(F32) * total[2].astype(BF).astype(F32)
        return 0

    lax.fori_loop(0, 4, project, 0)
    last = 4 * rows
    halo_next = remote(cin.at[pl.ds(last, 8)], cin.at[pl.ds(0, 8)], halo_s.at[0], halo_r.at[0], (me + 1) % 32, x)
    halo_prev = remote(cin.at[pl.ds(8, 8)], cin.at[pl.ds(last + 8, 8)], halo_s.at[1], halo_r.at[1], (me + 31) % 32, x)
    halo_next.start()
    halo_prev.start()

    b_steps(0)
    a_steps(3)
    b_steps(1)
    b_steps(2)
    b_steps(3)

    halo_next.wait()
    halo_prev.wait()
    cin[0:8] = cin[0:8] * jnp.where(me > 0, 1.0, 0.0)
    cin[last + 8:last + 16] = cin[last + 8:last + 16] * jnp.where(me < 31, 1.0, 0.0)
    tap = taps[...].astype(F32)
    conv = tap[0:1] * cin[7:last + 7] + tap[1:2] * cin[8:last + 8] + tap[2:3] * cin[9:last + 9]
    mixed[...] = (gate_b[...].astype(F32) * conv).astype(BF)

    def drain(c, _):
        for copy in (
            tok_right, tok_left, tok_on_right, tok_on_left, mix_right, mix_left, mix_on_right, mix_on_left,
            b_all, b_right, b_left, b_on_right, b_on_left, a_all,
        ):
            copy(c).wait_send()
        return 0

    lax.fori_loop(0, NC, drain, 0)


def combine_kernel(
    hid_hbm, hid_b, metas, down_hbm, mixed, proj_hbm,
    out, mix_out,
    hid_a, down_w, proj_w, p_a, p_b, bh_in, bf_in, sum_b, ret_a, ret_b, w_a, w_b, p_t, th_in, tf_in, p_m, mh_in, mf_in,
    bh_s, bh_r, bf_s, bf_r, b_s, b_r, a_s, a_r, th_s, th_r, tf_s, tf_r, mh_s, mh_r, mf_s, mf_r, w_sem,
):
    me = lax.axis_index("ep")
    x = lax.axis_index("tp")
    right, left = (x + 1) % 4, (x + 3) % 4
    cw = p_a.shape[4]
    rows = p_t.shape[2]
    half = rows // 2
    hb = NB // 2
    down_in = pltpu.make_async_copy(down_hbm, down_w, w_sem.at[0])
    proj_in = pltpu.make_async_copy(proj_hbm, proj_w, w_sem.at[1])
    hid_in = pltpu.make_async_copy(hid_hbm, hid_a, w_sem.at[2])
    everyone_in = greet(me, x)
    down_in.start()
    hid_in.start()
    proj_in.start()

    def cols(c):
        return pl.ds(pl.multiple_of(c * cw, cw), cw)

    def ring(buf, halves, wholes, one_s, one_r, two_s, two_r):
        size = buf.shape[2] // 2
        top = buf.shape[1] - 1
        return (
            lambda c: remote(buf.at[c, top, pl.ds(0, size)], halves.at[c, 0], one_s.at[c, 0], one_r.at[c, 0], me, right),
            lambda c: remote(buf.at[c, top, pl.ds(size, size)], halves.at[c, 1], one_s.at[c, 1], one_r.at[c, 1], me, left),
            lambda c: remote(buf.at[c, top - 1], wholes.at[c, 0], two_s.at[c, 0], two_r.at[c, 0], me, right),
            lambda c: remote(buf.at[c, top - 2], wholes.at[c, 1], two_s.at[c, 1], two_r.at[c, 1], me, left),
        )

    b_ring = ring(p_b, bh_in, bf_in, bh_s, bh_r, bf_s, bf_r)
    t_ring = ring(p_t, th_in, tf_in, th_s, th_r, tf_s, tf_r)
    m_ring = ring(p_m, mh_in, mf_in, mh_s, mh_r, mf_s, mf_r)

    def open_ring(copies, c):
        copies[0](c).start()
        copies[1](c).start()

    def pass_on(copies, buf, halves, c):
        size = buf.shape[2] // 2
        top = buf.shape[1] - 1
        copies[0](c).wait_recv()
        buf[c, top - 1, :size] = (buf[c, top - 1, :size].astype(F32) + halves[c, 0].astype(F32)).astype(BF)
        copies[2](c).start()
        copies[1](c).wait_recv()
        buf[c, top - 2, size:] = (buf[c, top - 2, size:].astype(F32) + halves[c, 1].astype(F32)).astype(BF)
        copies[3](c).start()

    def arrivals(copies, wholes, c):
        copies[2](c).wait_recv()
        copies[3](c).wait_recv()
        return wholes[c, 0].astype(F32) + wholes[c, 1].astype(F32)

    def a_all(c):
        span = pl.ds(1, NA - 1)
        return remote(p_a.at[c, span], ret_a.at[c, span], a_s.at[c], a_r.at[c], me, right)

    def b_all(c):
        return remote(sum_b.at[c], ret_b.at[c], b_s.at[c], b_r.at[c], me, right)

    def down_b(c):
        def one(r, _):
            part = jnp.dot(hid_b[r].reshape(NB * SLOT, hid_b.shape[3]), down_w[:, cols(c)], preferred_element_type=F32)
            p_b[c, r] = part.astype(BF).reshape(NB, SLOT, cw)
            return 0

        lax.fori_loop(0, 4, one, 0)

    down_in.wait()
    down_b(0)
    everyone_in()
    open_ring(b_ring, 0)

    def first(c, _):
        down_b(c)
        open_ring(b_ring, c)
        return 0

    lax.fori_loop(1, NC, first, 0)
    hid_in.wait()

    def second(c, _):
        def one(t, _):
            span = pl.ds(t * PER, PER)
            values = hid_a[span].reshape(PER * 4 * SLOT, hid_a.shape[3])
            part = jnp.dot(values, down_w[:, cols(c)], preferred_element_type=F32)
            p_a[c, span] = part.astype(BF).reshape(PER, 4, SLOT, cw)
            return 0

        lax.fori_loop(0, NA // PER, one, 0)
        for o in range(1, NA):
            remote(p_a.at[c, o], ret_a.at[c, o], a_s.at[c], a_r.at[c], peer(me, NEAR[o], -1), x).start()
        ret_a[c, 0] = p_a[c, 0]
        pass_on(b_ring, p_b, bh_in, c)
        return 0

    lax.fori_loop(0, NC, second, 0)
    proj_in.wait()

    def mixer(c, _):
        def one(r, _):
            values = mixed[pl.ds(pl.multiple_of(place(x, r) * rows, rows), rows)]
            p_m[c, r] = jnp.dot(values, proj_w[:, cols(c)], preferred_element_type=F32).astype(BF)
            return 0

        lax.fori_loop(0, 4, one, 0)
        open_ring(m_ring, c)
        return 0

    lax.fori_loop(0, NC, mixer, 0)

    for o in range(NA):
        base = peer(me, NEAR[o], 1) * SLOT
        for r in range(4):
            meta = metas[r]
            w_a[r, o] = slot_rows(base, SLOT, meta, meta[2:3], meta[3:4]).astype(BF)
    for o in range(NB):
        meta = metas[0]
        w_b[o] = slot_rows(peer(me, FAR[o], 1) * SLOT, SLOT, meta, meta[2:3], meta[3:4]).astype(BF)

    def third(c, _):
        sum_b[c] = (p_b[c, 0].astype(F32) + arrivals(b_ring, bf_in, c)).astype(BF)
        for o in range(NB):
            remote(sum_b.at[c, o], ret_b.at[c, o], b_s.at[c], b_r.at[c], peer(me, FAR[o], -1), x).start()
        pass_on(m_ring, p_m, mh_in, c)
        return 0

    lax.fori_loop(0, NC, third, 0)
    over_rows = (((0,), (0,)), ((), ()))

    def weighed(r, c):
        values = ret_a[c, :, r].reshape(NA * SLOT, cw)
        return lax.dot_general(w_a[r].reshape(NA * SLOT, rows), values, over_rows, preferred_element_type=F32)

    def fourth(c, _):
        a_all(c).wait_recv()
        p_t[c, 2] = weighed(3, c).astype(BF)
        open_ring(t_ring, c)
        p_t[c, 0] = weighed(1, c).astype(BF)
        p_t[c, 1] = weighed(2, c).astype(BF)
        return 0

    lax.fori_loop(0, NC, fourth, 0)

    def fourth_on(c, _):
        pass_on(t_ring, p_t, th_in, c)
        return 0

    lax.fori_loop(0, NC, fourth_on, 0)

    def fifth(c, _):
        mix_out[:, cols(c)] = (p_m[c, 0].astype(F32) + arrivals(m_ring, mf_in, c)).astype(BF)
        return 0

    lax.fori_loop(0, NC, fifth, 0)

    def sixth(c, _):
        b_all(c).wait_recv()
        values = ret_b[c].reshape(NB * SLOT, cw)
        total = weighed(0, c) + lax.dot_general(
            w_b[...].reshape(NB * SLOT, rows), values, over_rows, preferred_element_type=F32
        )
        out[:, cols(c)] = (total + arrivals(t_ring, tf_in, c)).astype(BF)
        return 0

    lax.fori_loop(0, NC, sixth, 0)

    def drain(c, _):
        for copy in b_ring + t_ring + m_ring + (a_all, b_all):
            copy(c).wait_send()
        return 0

    lax.fori_loop(0, NC, drain, 0)


VM = pltpu.VMEM
DMA = pltpu.SemaphoreType.DMA
PARAMS = dict(has_side_effects=True, vmem_limit_bytes=64 * 1024 * 1024 - 65536)
COST = pl.CostEstimate(flops=100_000_000_000, bytes_accessed=12_000_000, transcendentals=0)


def specs(places):
    vmem = pl.BlockSpec(memory_space=VM)
    anywhere = pl.BlockSpec(memory_space=pl.ANY)
    return [vmem if place == "v" else anywhere for place in places]


def dispatch(moe_in, moe_gain, routes, group_logits, pair_logits, gate_mat, up_mat, mix_in, mix_gain, proj_b, proj_c, proj_h, taps):
    rows, width = moe_in.shape
    hidden = gate_mat.shape[1]
    chan = proj_b.shape[1]
    cw = width // NC
    pair = DMA((NC, 2))
    single = DMA((NC,))
    return pl.pallas_call(
        dispatch_kernel,
        name="dispatch",
        out_shape=(
            jax.ShapeDtypeStruct((NA, 4, SLOT, hidden), BF),
            jax.ShapeDtypeStruct((4, NB, SLOT, hidden), BF),
            jax.ShapeDtypeStruct((4, 8, rows), F32),
            jax.ShapeDtypeStruct((4 * rows, chan), BF),
        ),
        in_specs=specs("avvvvaaavaaav"),
        out_specs=tuple(specs("vvvv")),
        scratch_shapes=[
            VM((rows, width), BF),
            VM((NC, 4, rows, cw), BF),
            VM((NC, 4, rows, cw), BF),
            VM((4, 8, rows), F32),
            VM((4, NA, SLOT, rows), BF),
            VM((NB, SLOT, rows), BF),
            VM((NC, NA, 4, SLOT, cw), BF),
            VM((NC, NB, SLOT, cw), BF),
            VM((NC, NA, 4, SLOT, cw), BF),
            VM((NC, 4, NB, SLOT, cw), BF),
            VM((width, hidden), BF),
            VM((width, hidden), BF),
            VM((3, width, chan), BF),
            VM((NA // PER, PER * 4 * SLOT, hidden), F32),
            VM((NA // PER, PER * 4 * SLOT, hidden), F32),
            VM((4, NB * SLOT, hidden), F32),
            VM((4, NB * SLOT, hidden), F32),
            VM((4 * rows + 16, chan), F32),
            VM((4 * rows, chan), BF),
            pair, pair, pair, pair, pair, pair, pair, pair, single, single, pair, pair, pair, pair, single, single,
            DMA((3,)), DMA((3,)), DMA((2,)), DMA((2,)), DMA((7,)),
        ],
        compiler_params=pltpu.CompilerParams(collective_id=0, **PARAMS),
        cost_estimate=COST,
    )(moe_in, moe_gain, routes, group_logits, pair_logits, gate_mat, up_mat, mix_in, mix_gain, proj_b, proj_c, proj_h, taps)


def combine(hid_a, hid_b, metas, down_mat, mixed, proj_out):
    rows = metas.shape[2]
    hidden, width = down_mat.shape
    chan = proj_out.shape[0]
    cw = width // NC
    hb = NB // 2
    pair = DMA((NC, 2))
    single = DMA((NC,))
    return pl.pallas_call(
        combine_kernel,
        name="combine",
        out_shape=(jax.ShapeDtypeStruct((rows, width), BF), jax.ShapeDtypeStruct((rows, width), BF)),
        in_specs=specs("avvava"),
        out_specs=tuple(specs("vv")),
        scratch_shapes=[
            VM((NA, 4, SLOT, hidden), BF),
            VM((hidden, width), BF),
            VM((chan, width), BF),
            VM((NC, NA, 4, SLOT, cw), BF),
            VM((NC, 4, NB, SLOT, cw), BF),
            VM((NC, 2, hb, SLOT, cw), BF),
            VM((NC, 2, NB, SLOT, cw), BF),
            VM((NC, NB, SLOT, cw), BF),
            VM((NC, NA, 4, SLOT, cw), BF),
            VM((NC, NB, SLOT, cw), BF),
            VM((4, NA, SLOT, rows), BF),
            VM((NB, SLOT, rows), BF),
            VM((NC, 3, rows, cw), BF),
            VM((NC, 2, rows // 2, cw), BF),
            VM((NC, 2, rows, cw), BF),
            VM((NC, 4, rows, cw), BF),
            VM((NC, 2, rows // 2, cw), BF),
            VM((NC, 2, rows, cw), BF),
            pair, pair, pair, pair, single, single, single, single,
            pair, pair, pair, pair, pair, pair, pair, pair, DMA((3,)),
        ],
        compiler_params=pltpu.CompilerParams(collective_id=1, **PARAMS),
        cost_estimate=COST,
    )(hid_a, hid_b, metas, down_mat, mixed, proj_out)


def body(
    mix_in, mix_gain, proj_b, proj_c, proj_h, conv_taps, proj_out,
    moe_in, moe_gain, routes, group_logits, pair_logits, expert_gate, expert_up, expert_down,
):
    hid_a, hid_b, metas, mixed = dispatch(
        moe_in, moe_gain[None, :], routes.T, group_logits.T, pair_logits.T, expert_gate[0], expert_up[0],
        mix_in, mix_gain[None, :], proj_b, proj_c, proj_h, conv_taps,
    )
    moe_out, mix_out = combine(hid_a, hid_b, metas, expert_down[0], mixed, proj_out)
    return (mix_out, moe_out)


def solution(mesh):
    in_specs = (
        P(("ep", "tp"), None), P(), P(None, "tp"), P(None, "tp"), P(None, "tp"), P(None, "tp"), P("tp", None),
        P(("ep", "tp"), None), P(), P(("ep", "tp"), None), P(("ep", "tp"), None), P(("ep", "tp"), None),
        P("ep", None, "tp"), P("ep", None, "tp"), P("ep", "tp", None),
    )
    out_specs = (P(("ep", "tp"), None), P(("ep", "tp"), None))
    return jax.shard_map(body, mesh=mesh, in_specs=in_specs, out_specs=out_specs, check_vma=False)
```

```python
import jax
import jax.numpy as jnp
from jax import lax
from jax.experimental import pallas as pl
from jax.experimental.pallas import tpu as pltpu
from jax.sharding import PartitionSpec as P

GROUPS = 4
BF = jnp.bfloat16
F32 = jnp.float32
MESH = pl.DeviceIdType.MESH
SLOT = 16
CAP = 14
BLOCK = 4 * CAP
SPACE = 64
def both(*chips):
    return [(dz, dy, c) for dz, dy in chips for c in (0, 1)]


NEAR = both((0, 0), (1, 0), (3, 0), (0, 1), (0, 3), (2, 0), (0, 2), (1, 1), (3, 3), (1, 3), (3, 1))
FAR = both((2, 1), (2, 3), (1, 2), (3, 2), (2, 2))
NA = len(NEAR)
NB = len(FAR)
NC = 4
PER = 4


def place(x, r):
    return (x + (3 * ((r * (r + 1)) // 2)) % 4) % 4


def peer(me, offset, sign):
    z, y, c = me // 8, (me // 2) % 4, me % 2
    dz, dy, dc = offset
    return (((z + sign * dz + 4) % 4) * 4 + (y + sign * dy + 4) % 4) * 2 + (c + dc) % 2


def greet(me, x):
    barrier = pltpu.get_barrier_semaphore()
    for offset in NEAR[1:] + FAR:
        pl.semaphore_signal(barrier, inc=1, device_id=(peer(me, offset, 1), x), device_id_type=MESH)
    pl.semaphore_signal(barrier, inc=1, device_id=(me, (x + 1) % 4), device_id_type=MESH)
    pl.semaphore_signal(barrier, inc=1, device_id=(me, (x + 3) % 4), device_id_type=MESH)
    return lambda: pl.semaphore_wait(barrier, NA - 1 + NB + 2)


def remote(src, dst, send, recv, ep, tp):
    return pltpu.make_async_remote_copy(
        src_ref=src, dst_ref=dst, send_sem=send, recv_sem=recv, device_id=(ep, tp), device_id_type=MESH
    )


def slot_rows(base, rows, meta, hit0, hit1):
    want = lax.broadcasted_iota(jnp.int32, (rows, meta.shape[1]), 0) + base
    want = want.astype(F32)
    return jnp.where(meta[0:1] == want, hit0, 0.0) + jnp.where(meta[1:2] == want, hit1, 0.0)


def far_rows(me, o, meta, hit0, hit1):
    return slot_rows(peer(me, FAR[o], 1) * SPACE, SLOT, meta, hit0, hit1).astype(BF)


def near_rows(me, o, r, meta, hit0, hit1):
    return slot_rows(peer(me, NEAR[o], 1) * SPACE - CAP * r, BLOCK, meta, hit0, hit1).astype(BF)


def near_steps(do):
    def one(t, _):
        do(t * PER, PER)
        return 0

    lax.fori_loop(0, NA // PER, one, 0)
    if NA % PER:
        do(NA - NA % PER, NA % PER)


def routing(routes, group_logits, pair_logits):
    count = routes.shape[1]
    r0, r1 = routes[0:1], routes[1:2]
    expert = lax.broadcasted_iota(jnp.int32, (32, count), 0)
    hit0, hit1 = jnp.where(expert == r0, 1.0, 0.0), jnp.where(expert == r1, 1.0, 0.0)
    earlier = lax.broadcasted_iota(jnp.int32, (count, count), 0) < lax.broadcasted_iota(jnp.int32, (count, count), 1)
    before = jnp.dot((hit0 + hit1).astype(BF), jnp.where(earlier, 1.0, 0.0).astype(BF), preferred_element_type=F32)

    def share(logits):
        grown = jnp.exp(logits - jnp.max(logits, axis=0, keepdims=True))
        return grown / jnp.sum(grown, axis=0, keepdims=True)

    group, pair = share(group_logits), share(pair_logits)

    def one(route, hit, k):
        slot = route.astype(F32) * SPACE + jnp.sum(before * hit, axis=0, keepdims=True)
        member = sum(
            group[g:g + 1] * jnp.where(jnp.logical_and(route >= 8 * g, route < 8 * g + 8), 1.0, 0.0) for g in range(GROUPS)
        )
        return slot, member * pair[k:k + 1]

    slot0, weight0 = one(r0, hit0, 0)
    slot1, weight1 = one(r1, hit1, 1)
    return jnp.concatenate([slot0, slot1, weight0, weight1, jnp.zeros((4, count), F32)], axis=0)


def normed(raw, gain, into, width):
    step = 16
    cw = into.shape[3]

    def one(t, _):
        span = pl.ds(pl.multiple_of(t * step, step), step)
        values = raw[span, :].astype(F32)
        scale = lax.rsqrt(jnp.sum(values * values, axis=1, keepdims=True) * (1.0 / width) + 1e-06)
        values = (values * scale * gain[...]).astype(BF)
        for c in range(NC):
            into[c, 0, span, :] = values[:, c * cw:(c + 1) * cw]
        return 0

    lax.fori_loop(0, raw.shape[0] // step, one, 0)


def dispatch_kernel(
    moe_hbm, moe_gain, routes, group_logits, pair_logits, gate_hbm, up_hbm, mix_hbm, mix_gain, projb_hbm, projc_hbm, projh_hbm, taps,
    hid_a, hid_b, metas_out, mixed,
    raw, tok, mix, metas, oh_a, oh_b, out_a, out_b, recv_a, recv_b, gate_w, up_w, proj_w,
    acc_g, acc_u, bcc_g, bcc_u, cin, gate_b,
    tok_s, tok_r, tokf_s, tokf_r, mx_s, mx_r, mxf_s, mxf_r, b_s, b_r, bx_s, bx_r, bf_s, bf_r, a_s, a_r,
    meta_s, meta_r, halo_s, halo_r, w_sem,
):
    me = lax.axis_index("ep")
    x = lax.axis_index("tp")
    right, left = (x + 1) % 4, (x + 3) % 4
    rows, cw = tok.shape[2], tok.shape[3]
    width = NC * cw
    half = rows // 2
    hb = NB // 2
    chan = gate_b.shape[1]
    moe_in = pltpu.make_async_copy(moe_hbm, raw, w_sem.at[0])
    mix_in = pltpu.make_async_copy(mix_hbm, raw, w_sem.at[1])
    loads = [
        pltpu.make_async_copy(gate_hbm, gate_w, w_sem.at[2]),
        pltpu.make_async_copy(up_hbm, up_w, w_sem.at[3]),
        pltpu.make_async_copy(projb_hbm, proj_w.at[0], w_sem.at[4]),
        pltpu.make_async_copy(projc_hbm, proj_w.at[1], w_sem.at[5]),
        pltpu.make_async_copy(projh_hbm, proj_w.at[2], w_sem.at[6]),
    ]
    moe_in.start()
    everyone_in = greet(me, x)
    for load in loads:
        load.start()
    metas[0] = routing(routes[...], group_logits[...], pair_logits[...])
    moe_in.wait()
    normed(raw, moe_gain, tok, width)
    mix_in.start()
    everyone_in()

    meta_right = remote(metas.at[0], metas.at[1], meta_s.at[0], meta_r.at[0], me, right)
    meta_left = remote(metas.at[0], metas.at[2], meta_s.at[1], meta_r.at[1], me, left)
    meta_on = remote(metas.at[1], metas.at[3], meta_s.at[2], meta_r.at[2], me, right)
    meta_right.start()
    meta_left.start()

    def ring(buf, one_s, one_r, two_s, two_r):
        size = buf.shape[2] // 2
        lo, hi = pl.ds(0, size), pl.ds(size, size)
        return (
            lambda c: remote(buf.at[c, 0], buf.at[c, 1], one_s.at[c, 0], one_r.at[c, 0], me, right),
            lambda c: remote(buf.at[c, 0], buf.at[c, 2], one_s.at[c, 1], one_r.at[c, 1], me, left),
            lambda c: remote(buf.at[c, 1, lo], buf.at[c, 3, lo], two_s.at[c, 0], two_r.at[c, 0], me, right),
            lambda c: remote(buf.at[c, 2, hi], buf.at[c, 3, hi], two_s.at[c, 1], two_r.at[c, 1], me, left),
        )

    tok_right, tok_left, tok_on_right, tok_on_left = ring(tok, tok_s, tok_r, tokf_s, tokf_r)
    mix_right, mix_left, mix_on_right, mix_on_left = ring(mix, mx_s, mx_r, mxf_s, mxf_r)
    b_right, b_left, b_on_right, b_on_left = ring(recv_b, bx_s, bx_r, bf_s, bf_r)

    def a_all(c):
        span = pl.ds(1, NA - 1)
        return remote(out_a.at[c, span], recv_a.at[c, span], a_s.at[c], a_r.at[c], me, right)

    def b_all(c):
        return remote(out_b.at[c], recv_b.at[c, 0], b_s.at[c], b_r.at[c], me, right)

    def first(c, _):
        tok_right(c).start()
        tok_left(c).start()
        return 0

    lax.fori_loop(0, NC, first, 0)

    own = metas[0]
    for o in range(NB):
        oh_b[o] = far_rows(me, o, own, 1.0, 1.0)

    def second(c, _):
        picked = jnp.dot(oh_b[...].reshape(NB * SLOT, rows), tok[c, 0], preferred_element_type=F32)
        out_b[c] = picked.astype(BF).reshape(NB, SLOT, cw)
        for o in range(NB):
            remote(out_b.at[c, o], recv_b.at[c, 0, o], b_s.at[c], b_r.at[c], peer(me, FAR[o], 1), x).start()
        return 0

    lax.fori_loop(0, NC, second, 0)

    meta_right.wait()
    meta_on.start()
    meta_left.wait()
    meta_on.wait()
    metas_out[...] = metas[...]
    for o in range(NA):
        for r in range(4):
            oh_a[o, :, r * rows:(r + 1) * rows] = near_rows(me, o, r, metas_out[r], 1.0, 1.0)
    mix_in.wait()
    normed(raw, mix_gain, mix, width)

    def pick(c):
        def one(first, count):
            span = pl.ds(first, count)
            rows_in = oh_a[span].reshape(count * BLOCK, 4 * rows)
            picked = jnp.dot(rows_in, tok[c].reshape(4 * rows, cw), preferred_element_type=F32)
            out_a[c, span] = picked.astype(BF).reshape(count, BLOCK, cw)

        near_steps(one)

    def third(c, _):
        tok_right(c).wait_recv()
        tok_on_right(c).start()
        tok_left(c).wait_recv()
        tok_on_left(c).start()
        return 0

    lax.fori_loop(0, NC, third, 0)

    def mix_first(c, _):
        mix_right(c).start()
        mix_left(c).start()
        return 0

    lax.fori_loop(0, NC, mix_first, 0)

    def fourth(c, _):
        tok_on_right(c).wait_recv()
        tok_on_left(c).wait_recv()
        pick(c)
        for o in range(1, NA):
            remote(out_a.at[c, o], recv_a.at[c, o], a_s.at[c], a_r.at[c], peer(me, NEAR[o], 1), x).start()
        recv_a[c, 0] = out_a[c, 0]
        return 0

    lax.fori_loop(0, NC, fourth, 0)

    def b_first(c, _):
        b_all(c).wait_recv()
        b_right(c).start()
        b_left(c).start()
        return 0

    lax.fori_loop(0, NC, b_first, 0)

    def mix_second(c, _):
        mix_right(c).wait_recv()
        mix_on_right(c).start()
        mix_left(c).wait_recv()
        mix_on_left(c).start()
        return 0

    lax.fori_loop(0, NC, mix_second, 0)

    def b_second(c):
        b_right(c).wait_recv()
        b_on_right(c).start()
        b_left(c).wait_recv()
        b_on_left(c).start()

    for load in loads:
        load.wait()

    def finish(gate_val, up_val):
        return (gate_val / (1.0 + jnp.exp(-gate_val)) * up_val).astype(BF)

    def chunk_dots(values, mats, c):
        return [jnp.dot(values, mat[c * cw:(c + 1) * cw], preferred_element_type=F32) for mat in mats]

    def step(c, values, sums, at, store):
        g, u = chunk_dots(values, (gate_w, up_w), c)
        if c > 0:
            g = g + sums[0][at]
            u = u + sums[1][at]
        if c < NC - 1:
            sums[0][at] = g
            sums[1][at] = u
        else:
            store[at] = finish(g, u)

    def a_steps(c):
        a_all(c).wait_recv()

        def one(first, count):
            values = recv_a[c, pl.ds(first, count)].reshape(count * BLOCK, cw)
            step(c, values, (acc_g, acc_u), pl.ds(pl.multiple_of(first * BLOCK, BLOCK), count * BLOCK), hid_a)

        near_steps(one)

    def b_steps(c):
        b_on_right(c).wait_recv()
        b_on_left(c).wait_recv()

        def one(r, _):
            step(c, recv_b[c, r].reshape(NB * SLOT, cw), (bcc_g, bcc_u), r, hid_b)
            return 0

        lax.fori_loop(0, 4, one, 0)

    a_steps(0)
    b_second(0)
    a_steps(1)
    b_second(1)
    b_second(2)
    a_steps(2)
    b_second(3)

    for c in range(NC):
        mix_on_right(c).wait_recv()
        mix_on_left(c).wait_recv()

    def project(r, _):
        start = pl.multiple_of(place(x, r) * rows, rows)
        total = None
        for c in range(NC):
            parts = chunk_dots(mix[c, r], [proj_w.at[n] for n in range(3)], c)
            total = parts if total is None else [one + two for one, two in zip(total, parts)]
        gate_b[pl.ds(start, rows)] = total[0].astype(BF)
        cin[pl.ds(start + 8, rows)] = total[1].astype(BF).astype(F32) * total[2].astype(BF).astype(F32)
        return 0

    lax.fori_loop(0, 4, project, 0)
    last = 4 * rows
    halo_next = remote(cin.at[pl.ds(last, 8)], cin.at[pl.ds(0, 8)], halo_s.at[0], halo_r.at[0], (me + 1) % 32, x)
    halo_prev = remote(cin.at[pl.ds(8, 8)], cin.at[pl.ds(last + 8, 8)], halo_s.at[1], halo_r.at[1], (me + 31) % 32, x)
    halo_next.start()
    halo_prev.start()

    b_steps(0)
    b_steps(1)
    b_steps(2)
    halo_next.wait()
    halo_prev.wait()
    cin[0:8] = cin[0:8] * jnp.where(me > 0, 1.0, 0.0)
    cin[last + 8:last + 16] = cin[last + 8:last + 16] * jnp.where(me < 31, 1.0, 0.0)
    tap = taps[...].astype(F32)
    conv = tap[0:1] * cin[7:last + 7] + tap[1:2] * cin[8:last + 8] + tap[2:3] * cin[9:last + 9]
    mixed[...] = (gate_b[...].astype(F32) * conv).astype(BF)

    b_steps(3)
    a_steps(3)

    def drain(c, _):
        for copy in (
            tok_right, tok_left, tok_on_right, tok_on_left, mix_right, mix_left, mix_on_right, mix_on_left,
            b_all, b_right, b_left, b_on_right, b_on_left, a_all,
        ):
            copy(c).wait_send()
        return 0

    lax.fori_loop(0, NC, drain, 0)


def combine_kernel(
    hid_hbm, hid_b, metas, down_hbm, mixed, proj_hbm,
    out, mix_out,
    hid_a, down_w, proj_w, p_a, p_b, bh_in, bf_in, sum_b, ret_a, ret_b, w_a, w_b, p_t, th_in, tf_in, p_m, mh_in, mf_in, acc,
    bh_s, bh_r, bf_s, bf_r, b_s, b_r, a_s, a_r, th_s, th_r, tf_s, tf_r, mh_s, mh_r, mf_s, mf_r, w_sem,
):
    me = lax.axis_index("ep")
    x = lax.axis_index("tp")
    right, left = (x + 1) % 4, (x + 3) % 4
    cw = p_a.shape[3]
    rows = p_t.shape[2]
    half = rows // 2
    hb = NB // 2
    down_in = pltpu.make_async_copy(down_hbm, down_w, w_sem.at[0])
    proj_in = pltpu.make_async_copy(proj_hbm, proj_w, w_sem.at[1])
    hid_in = pltpu.make_async_copy(hid_hbm, hid_a, w_sem.at[2])
    everyone_in = greet(me, x)
    down_in.start()
    hid_in.start()
    proj_in.start()

    def cols(c):
        return pl.ds(pl.multiple_of(c * cw, cw), cw)

    def ring(buf, halves, wholes, one_s, one_r, two_s, two_r):
        size = buf.shape[2] // 2
        top = buf.shape[1] - 1
        return (
            lambda c: remote(buf.at[c, top, pl.ds(0, size)], halves.at[c, 0], one_s.at[c, 0], one_r.at[c, 0], me, right),
            lambda c: remote(buf.at[c, top, pl.ds(size, size)], halves.at[c, 1], one_s.at[c, 1], one_r.at[c, 1], me, left),
            lambda c: remote(buf.at[c, top - 1], wholes.at[c, 0], two_s.at[c, 0], two_r.at[c, 0], me, right),
            lambda c: remote(buf.at[c, top - 2], wholes.at[c, 1], two_s.at[c, 1], two_r.at[c, 1], me, left),
        )

    b_ring = ring(p_b, bh_in, bf_in, bh_s, bh_r, bf_s, bf_r)
    t_ring = ring(p_t, th_in, tf_in, th_s, th_r, tf_s, tf_r)
    m_ring = ring(p_m, mh_in, mf_in, mh_s, mh_r, mf_s, mf_r)

    def open_ring(copies, c):
        copies[0](c).start()
        copies[1](c).start()

    def pass_on(copies, buf, halves, c):
        size = buf.shape[2] // 2
        top = buf.shape[1] - 1
        copies[0](c).wait_recv()
        buf[c, top - 1, :size] = (buf[c, top - 1, :size].astype(F32) + halves[c, 0].astype(F32)).astype(BF)
        copies[2](c).start()
        copies[1](c).wait_recv()
        buf[c, top - 2, size:] = (buf[c, top - 2, size:].astype(F32) + halves[c, 1].astype(F32)).astype(BF)
        copies[3](c).start()

    def arrivals(copies, wholes, c):
        copies[2](c).wait_recv()
        copies[3](c).wait_recv()
        return wholes[c, 0].astype(F32) + wholes[c, 1].astype(F32)

    def a_all(c):
        span = pl.ds(1, NA - 1)
        return remote(p_a.at[c, span], ret_a.at[c, span], a_s.at[c], a_r.at[c], me, right)

    def b_all(c):
        return remote(sum_b.at[c], ret_b.at[c], b_s.at[c], b_r.at[c], me, right)

    def down_b(c):
        def one(r, _):
            part = jnp.dot(hid_b[r], down_w[:, cols(c)], preferred_element_type=F32)
            p_b[c, r] = part.astype(BF).reshape(NB, SLOT, cw)
            return 0

        lax.fori_loop(0, 4, one, 0)

    down_in.wait()
    down_b(0)
    everyone_in()
    open_ring(b_ring, 0)
    hid_in.wait()

    def down_a(c):
        def one(first, count):
            values = hid_a[pl.ds(pl.multiple_of(first * BLOCK, BLOCK), count * BLOCK)]
            part = jnp.dot(values, down_w[:, cols(c)], preferred_element_type=F32)
            p_a[c, pl.ds(first, count)] = part.astype(BF).reshape(count, BLOCK, cw)

        near_steps(one)
        for o in range(1, NA):
            remote(p_a.at[c, o], ret_a.at[c, o], a_s.at[c], a_r.at[c], peer(me, NEAR[o], -1), x).start()
        ret_a[c, 0] = p_a[c, 0]

    down_a(0)

    def first(c, _):
        down_b(c)
        open_ring(b_ring, c)
        return 0

    lax.fori_loop(1, NC, first, 0)
    pass_on(b_ring, p_b, bh_in, 0)

    def second(c, _):
        down_a(c)
        pass_on(b_ring, p_b, bh_in, c)
        return 0

    lax.fori_loop(1, NC, second, 0)
    proj_in.wait()

    def mixer(c, _):
        def one(r, _):
            values = mixed[pl.ds(pl.multiple_of(place(x, r) * rows, rows), rows)]
            p_m[c, r] = jnp.dot(values, proj_w[:, cols(c)], preferred_element_type=F32).astype(BF)
            return 0

        lax.fori_loop(0, 4, one, 0)
        open_ring(m_ring, c)
        return 0

    lax.fori_loop(0, NC, mixer, 0)

    for o in range(NA):
        for r in range(4):
            meta = metas[r]
            w_a[r, o] = near_rows(me, o, r, meta, meta[2:3], meta[3:4])
    for o in range(NB):
        meta = metas[0]
        w_b[o] = far_rows(me, o, meta, meta[2:3], meta[3:4])

    def third(c, _):
        sum_b[c] = (p_b[c, 0].astype(F32) + arrivals(b_ring, bf_in, c)).astype(BF)
        for o in range(NB):
            remote(sum_b.at[c, o], ret_b.at[c, o], b_s.at[c], b_r.at[c], peer(me, FAR[o], -1), x).start()
        pass_on(m_ring, p_m, mh_in, c)
        return 0

    lax.fori_loop(0, NC, third, 0)
    over_rows = (((0,), (0,)), ((), ()))

    def weighed(r, c):
        values = ret_a[c].reshape(NA * BLOCK, cw)
        return lax.dot_general(w_a[r].reshape(NA * BLOCK, rows), values, over_rows, preferred_element_type=F32)

    def fourth(c, _):
        a_all(c).wait_recv()
        p_t[c, 2] = weighed(3, c).astype(BF)
        open_ring(t_ring, c)
        p_t[c, 0] = weighed(1, c).astype(BF)
        p_t[c, 1] = weighed(2, c).astype(BF)
        acc[c] = weighed(0, c)
        return 0

    lax.fori_loop(0, NC, fourth, 0)

    def fourth_on(c, _):
        pass_on(t_ring, p_t, th_in, c)
        return 0

    lax.fori_loop(0, NC, fourth_on, 0)

    def fifth(c, _):
        mix_out[:, cols(c)] = (p_m[c, 0].astype(F32) + arrivals(m_ring, mf_in, c)).astype(BF)
        return 0

    lax.fori_loop(0, NC, fifth, 0)

    def sixth(c, _):
        b_all(c).wait_recv()
        values = ret_b[c].reshape(NB * SLOT, cw)
        total = acc[c] + lax.dot_general(
            w_b[...].reshape(NB * SLOT, rows), values, over_rows, preferred_element_type=F32
        )
        out[:, cols(c)] = (total + arrivals(t_ring, tf_in, c)).astype(BF)
        return 0

    lax.fori_loop(0, NC, sixth, 0)

    def drain(c, _):
        for copy in b_ring + t_ring + m_ring + (a_all, b_all):
            copy(c).wait_send()
        return 0

    lax.fori_loop(0, NC, drain, 0)


VM = pltpu.VMEM
DMA = pltpu.SemaphoreType.DMA
PARAMS = dict(has_side_effects=True, vmem_limit_bytes=64 * 1024 * 1024 - 65536)
COST = pl.CostEstimate(flops=100_000_000_000, bytes_accessed=12_000_000, transcendentals=0)


def specs(places):
    vmem = pl.BlockSpec(memory_space=VM)
    anywhere = pl.BlockSpec(memory_space=pl.ANY)
    return [vmem if place == "v" else anywhere for place in places]


def dispatch(moe_in, moe_gain, routes, group_logits, pair_logits, gate_mat, up_mat, mix_in, mix_gain, proj_b, proj_c, proj_h, taps):
    rows, width = moe_in.shape
    hidden = gate_mat.shape[1]
    chan = proj_b.shape[1]
    cw = width // NC
    pair = DMA((NC, 2))
    single = DMA((NC,))
    return pl.pallas_call(
        dispatch_kernel,
        name="dispatch",
        out_shape=(
            jax.ShapeDtypeStruct((NA * BLOCK, hidden), BF),
            jax.ShapeDtypeStruct((4, NB * SLOT, hidden), BF),
            jax.ShapeDtypeStruct((4, 8, rows), F32),
            jax.ShapeDtypeStruct((4 * rows, chan), BF),
        ),
        in_specs=specs("avvvvaaavaaav"),
        out_specs=tuple(specs("vvvv")),
        scratch_shapes=[
            VM((rows, width), BF),
            VM((NC, 4, rows, cw), BF),
            VM((NC, 4, rows, cw), BF),
            VM((4, 8, rows), F32),
            VM((NA, BLOCK, 4 * rows), BF),
            VM((NB, SLOT, rows), BF),
            VM((NC, NA, BLOCK, cw), BF),
            VM((NC, NB, SLOT, cw), BF),
            VM((NC, NA, BLOCK, cw), BF),
            VM((NC, 4, NB, SLOT, cw), BF),
            VM((width, hidden), BF),
            VM((width, hidden), BF),
            VM((3, width, chan), BF),
            VM((NA * BLOCK, hidden), F32),
            VM((NA * BLOCK, hidden), F32),
            VM((4, NB * SLOT, hidden), F32),
            VM((4, NB * SLOT, hidden), F32),
            VM((4 * rows + 16, chan), F32),
            VM((4 * rows, chan), BF),
            pair, pair, pair, pair, pair, pair, pair, pair, single, single, pair, pair, pair, pair, single, single,
            DMA((3,)), DMA((3,)), DMA((2,)), DMA((2,)), DMA((7,)),
        ],
        compiler_params=pltpu.CompilerParams(collective_id=0, **PARAMS),
        cost_estimate=COST,
    )(moe_in, moe_gain, routes, group_logits, pair_logits, gate_mat, up_mat, mix_in, mix_gain, proj_b, proj_c, proj_h, taps)


def combine(hid_a, hid_b, metas, down_mat, mixed, proj_out):
    rows = metas.shape[2]
    hidden, width = down_mat.shape
    chan = proj_out.shape[0]
    cw = width // NC
    hb = NB // 2
    pair = DMA((NC, 2))
    single = DMA((NC,))
    return pl.pallas_call(
        combine_kernel,
        name="combine",
        out_shape=(jax.ShapeDtypeStruct((rows, width), BF), jax.ShapeDtypeStruct((rows, width), BF)),
        in_specs=specs("avvava"),
        out_specs=tuple(specs("vv")),
        scratch_shapes=[
            VM((NA * BLOCK, hidden), BF),
            VM((hidden, width), BF),
            VM((chan, width), BF),
            VM((NC, NA, BLOCK, cw), BF),
            VM((NC, 4, NB, SLOT, cw), BF),
            VM((NC, 2, hb, SLOT, cw), BF),
            VM((NC, 2, NB, SLOT, cw), BF),
            VM((NC, NB, SLOT, cw), BF),
            VM((NC, NA, BLOCK, cw), BF),
            VM((NC, NB, SLOT, cw), BF),
            VM((4, NA, BLOCK, rows), BF),
            VM((NB, SLOT, rows), BF),
            VM((NC, 3, rows, cw), BF),
            VM((NC, 2, rows // 2, cw), BF),
            VM((NC, 2, rows, cw), BF),
            VM((NC, 4, rows, cw), BF),
            VM((NC, 2, rows // 2, cw), BF),
            VM((NC, 2, rows, cw), BF),
            VM((NC, rows, cw), F32),
            pair, pair, pair, pair, single, single, single, single,
            pair, pair, pair, pair, pair, pair, pair, pair, DMA((3,)),
        ],
        compiler_params=pltpu.CompilerParams(collective_id=1, **PARAMS),
        cost_estimate=COST,
    )(hid_a, hid_b, metas, down_mat, mixed, proj_out)


def body(
    mix_in, mix_gain, proj_b, proj_c, proj_h, conv_taps, proj_out,
    moe_in, moe_gain, routes, group_logits, pair_logits, expert_gate, expert_up, expert_down,
):
    hid_a, hid_b, metas, mixed = dispatch(
        moe_in, moe_gain[None, :], routes.T, group_logits.T, pair_logits.T, expert_gate[0], expert_up[0],
        mix_in, mix_gain[None, :], proj_b, proj_c, proj_h, conv_taps,
    )
    moe_out, mix_out = combine(hid_a, hid_b, metas, expert_down[0], mixed, proj_out)
    return (mix_out, moe_out)


def solution(mesh):
    in_specs = (
        P(("ep", "tp"), None), P(), P(None, "tp"), P(None, "tp"), P(None, "tp"), P(None, "tp"), P("tp", None),
        P(("ep", "tp"), None), P(), P(("ep", "tp"), None), P(("ep", "tp"), None), P(("ep", "tp"), None),
        P("ep", None, "tp"), P("ep", None, "tp"), P("ep", "tp", None),
    )
    out_specs = (P(("ep", "tp"), None), P(("ep", "tp"), None))
    return jax.shard_map(body, mesh=mesh, in_specs=in_specs, out_specs=out_specs, check_vma=False)
```

```python
import jax
import jax.numpy as jnp
from jax import lax
from jax.experimental import pallas as pl
from jax.experimental.pallas import tpu as pltpu
from jax.sharding import PartitionSpec as P

GROUPS = 4
BF = jnp.bfloat16
F32 = jnp.float32
MESH = pl.DeviceIdType.MESH
SLOT = 16
CAP = 14
BLOCK = 4 * CAP
SPLIT = 14
SPACE = 64
def both(*chips):
    return [(dz, dy, c) for dz, dy in chips for c in (0, 1)]


NEAR = both((0, 0), (1, 0), (3, 0), (0, 1), (0, 3), (2, 0), (0, 2), (1, 1), (3, 3), (1, 3), (3, 1))
FAR = both((2, 1), (2, 3), (1, 2), (3, 2), (2, 2))
NA = len(NEAR)
NB = len(FAR)
NC = 4
PER = 6


def place(x, r):
    return (x + (3 * ((r * (r + 1)) // 2)) % 4) % 4


def peer(me, offset, sign):
    z, y, c = me // 8, (me // 2) % 4, me % 2
    dz, dy, dc = offset
    return (((z + sign * dz + 4) % 4) * 4 + (y + sign * dy + 4) % 4) * 2 + (c + dc) % 2


def greet(me, x):
    barrier = pltpu.get_barrier_semaphore()
    for offset in NEAR[1:] + FAR:
        pl.semaphore_signal(barrier, inc=1, device_id=(peer(me, offset, 1), x), device_id_type=MESH)
    pl.semaphore_signal(barrier, inc=1, device_id=(me, (x + 1) % 4), device_id_type=MESH)
    pl.semaphore_signal(barrier, inc=1, device_id=(me, (x + 3) % 4), device_id_type=MESH)
    return lambda: pl.semaphore_wait(barrier, NA - 1 + NB + 2)


def remote(src, dst, send, recv, ep, tp):
    return pltpu.make_async_remote_copy(
        src_ref=src, dst_ref=dst, send_sem=send, recv_sem=recv, device_id=(ep, tp), device_id_type=MESH
    )


def slot_rows(base, rows, meta, hit0, hit1):
    want = lax.broadcasted_iota(jnp.int32, (rows, meta.shape[1]), 0) + base
    want = want.astype(F32)
    return jnp.where(meta[0:1] == want, hit0, 0.0) + jnp.where(meta[1:2] == want, hit1, 0.0)


def far_rows(me, o, meta, hit0, hit1):
    return slot_rows(peer(me, FAR[o], 1) * SPACE, SLOT, meta, hit0, hit1).astype(BF)


def near_rows(me, o, r, meta, hit0, hit1):
    return slot_rows(peer(me, NEAR[o], 1) * SPACE - CAP * r, BLOCK, meta, hit0, hit1).astype(BF)


def near_steps(do):
    def one(t, _):
        do(t * PER, PER)
        return 0

    lax.fori_loop(0, NA // PER, one, 0)
    if NA % PER:
        do(NA - NA % PER, NA % PER)


def routing(routes, group_logits, pair_logits):
    count = routes.shape[1]
    r0, r1 = routes[0:1], routes[1:2]
    expert = lax.broadcasted_iota(jnp.int32, (32, count), 0)
    hit0, hit1 = jnp.where(expert == r0, 1.0, 0.0), jnp.where(expert == r1, 1.0, 0.0)
    earlier = lax.broadcasted_iota(jnp.int32, (count, count), 0) < lax.broadcasted_iota(jnp.int32, (count, count), 1)
    before = jnp.dot((hit0 + hit1).astype(BF), jnp.where(earlier, 1.0, 0.0).astype(BF), preferred_element_type=F32)

    def share(logits):
        grown = jnp.exp(logits - jnp.max(logits, axis=0, keepdims=True))
        return grown / jnp.sum(grown, axis=0, keepdims=True)

    group, pair = share(group_logits), share(pair_logits)

    def one(route, hit, k):
        slot = route.astype(F32) * SPACE + jnp.sum(before * hit, axis=0, keepdims=True)
        member = sum(
            group[g:g + 1] * jnp.where(jnp.logical_and(route >= 8 * g, route < 8 * g + 8), 1.0, 0.0) for g in range(GROUPS)
        )
        return slot, member * pair[k:k + 1]

    slot0, weight0 = one(r0, hit0, 0)
    slot1, weight1 = one(r1, hit1, 1)
    return jnp.concatenate([slot0, slot1, weight0, weight1, jnp.zeros((4, count), F32)], axis=0)


def normed(raw, gain, into, width):
    step = 16
    cw = into.shape[3]

    def one(t, _):
        span = pl.ds(pl.multiple_of(t * step, step), step)
        values = raw[span, :].astype(F32)
        scale = lax.rsqrt(jnp.sum(values * values, axis=1, keepdims=True) * (1.0 / width) + 1e-06)
        values = (values * scale * gain[...]).astype(BF)
        for c in range(NC):
            into[c, 0, span, :] = values[:, c * cw:(c + 1) * cw]
        return 0

    lax.fori_loop(0, raw.shape[0] // step, one, 0)


def dispatch_kernel(
    moe_hbm, moe_gain, routes, group_logits, pair_logits, gate_hbm, up_hbm, mix_hbm, mix_gain, projb_hbm, projc_hbm, projh_hbm, taps,
    hid_a, hid_b, metas_out, mixed,
    raw, tok, mix, metas, oh_a, oh_b, out_a, out_b, recv_a, recv_b, gate_w, up_w, proj_w,
    acc_g, acc_u, bcc_g, bcc_u, cin, gate_b,
    tok_s, tok_r, tokf_s, tokf_r, mx_s, mx_r, mxf_s, mxf_r, b_s, b_r, bx_s, bx_r, bf_s, bf_r, a_s, a_r,
    meta_s, meta_r, halo_s, halo_r, w_sem,
):
    me = lax.axis_index("ep")
    x = lax.axis_index("tp")
    right, left = (x + 1) % 4, (x + 3) % 4
    rows, cw = tok.shape[2], tok.shape[3]
    width = NC * cw
    half = rows // 2
    hb = NB // 2
    chan = gate_b.shape[1]
    moe_in = pltpu.make_async_copy(moe_hbm, raw, w_sem.at[0])
    mix_in = pltpu.make_async_copy(mix_hbm, raw, w_sem.at[1])
    loads = [
        pltpu.make_async_copy(gate_hbm, gate_w, w_sem.at[2]),
        pltpu.make_async_copy(up_hbm, up_w, w_sem.at[3]),
        pltpu.make_async_copy(projb_hbm, proj_w.at[0], w_sem.at[4]),
        pltpu.make_async_copy(projc_hbm, proj_w.at[1], w_sem.at[5]),
        pltpu.make_async_copy(projh_hbm, proj_w.at[2], w_sem.at[6]),
    ]
    moe_in.start()
    everyone_in = greet(me, x)
    for load in loads:
        load.start()
    metas[0] = routing(routes[...], group_logits[...], pair_logits[...])
    moe_in.wait()
    normed(raw, moe_gain, tok, width)
    mix_in.start()
    for o in range(NB):
        oh_b[o] = far_rows(me, o, metas[0], 1.0, 1.0)
    everyone_in()

    meta_right = remote(metas.at[0], metas.at[1], meta_s.at[0], meta_r.at[0], me, right)
    meta_left = remote(metas.at[0], metas.at[2], meta_s.at[1], meta_r.at[1], me, left)
    meta_on = remote(metas.at[1], metas.at[3], meta_s.at[2], meta_r.at[2], me, right)
    meta_right.start()
    meta_left.start()

    def ring(buf, one_s, one_r, two_s, two_r):
        size = buf.shape[2] // 2
        lo, hi = pl.ds(0, size), pl.ds(size, size)
        return (
            lambda c: remote(buf.at[c, 0], buf.at[c, 1], one_s.at[c, 0], one_r.at[c, 0], me, right),
            lambda c: remote(buf.at[c, 0], buf.at[c, 2], one_s.at[c, 1], one_r.at[c, 1], me, left),
            lambda c: remote(buf.at[c, 1, lo], buf.at[c, 3, lo], two_s.at[c, 0], two_r.at[c, 0], me, right),
            lambda c: remote(buf.at[c, 2, hi], buf.at[c, 3, hi], two_s.at[c, 1], two_r.at[c, 1], me, left),
        )

    tok_right, tok_left, tok_on_right, tok_on_left = ring(tok, tok_s, tok_r, tokf_s, tokf_r)
    mix_right, mix_left, mix_on_right, mix_on_left = ring(mix, mx_s, mx_r, mxf_s, mxf_r)
    b_right, b_left, b_on_right, b_on_left = ring(recv_b, bx_s, bx_r, bf_s, bf_r)

    def a_part(c, part):
        span = pl.ds(SPLIT, NA - SPLIT) if part else pl.ds(1, SPLIT - 1)
        return remote(out_a.at[c, span], recv_a.at[c, span], a_s.at[c, part], a_r.at[c, part], me, right)

    def b_all(c):
        return remote(out_b.at[c], recv_b.at[c, 0], b_s.at[c], b_r.at[c], me, right)

    def first(c, _):
        tok_right(c).start()
        tok_left(c).start()
        return 0

    lax.fori_loop(0, NC - 1, first, 0)

    def second(c, _):
        picked = jnp.dot(oh_b[...].reshape(NB * SLOT, rows), tok[c, 0], preferred_element_type=F32)
        out_b[c] = picked.astype(BF).reshape(NB, SLOT, cw)
        for o in range(NB):
            remote(out_b.at[c, o], recv_b.at[c, 0, o], b_s.at[c], b_r.at[c], peer(me, FAR[o], 1), x).start()
        return 0

    lax.fori_loop(0, NC, second, 0)

    meta_right.wait()
    meta_on.start()
    meta_left.wait()
    meta_on.wait()
    metas_out[...] = metas[...]
    for o in range(NA):
        for r in range(4):
            oh_a[o, :, r * rows:(r + 1) * rows] = near_rows(me, o, r, metas_out[r], 1.0, 1.0)

    def pick(c):
        def one(first, count):
            span = pl.ds(first, count)
            rows_in = oh_a[span].reshape(count * BLOCK, 4 * rows)
            picked = jnp.dot(rows_in, tok[c].reshape(4 * rows, cw), preferred_element_type=F32)
            out_a[c, span] = picked.astype(BF).reshape(count, BLOCK, cw)

        near_steps(one)

    def third(c, _):
        tok_right(c).wait_recv()
        tok_on_right(c).start()
        tok_left(c).wait_recv()
        tok_on_left(c).start()
        return 0

    third(0, 0)
    first(NC - 1, 0)
    lax.fori_loop(1, NC, third, 0)

    mix_in.wait()
    normed(raw, mix_gain, mix, width)

    def mix_first(c, _):
        mix_right(c).start()
        mix_left(c).start()
        return 0

    lax.fori_loop(0, NC, mix_first, 0)

    def fourth(c, _):
        tok_on_right(c).wait_recv()
        tok_on_left(c).wait_recv()
        pick(c)
        for o in range(1, NA):
            remote(
                out_a.at[c, o], recv_a.at[c, o], a_s.at[c, o // SPLIT], a_r.at[c, o // SPLIT], peer(me, NEAR[o], 1), x
            ).start()
        recv_a[c, 0] = out_a[c, 0]
        return 0

    lax.fori_loop(0, NC, fourth, 0)

    def b_first(c, _):
        b_all(c).wait_recv()
        b_right(c).start()
        b_left(c).start()
        return 0

    lax.fori_loop(0, NC, b_first, 0)

    def mix_second(c, _):
        mix_right(c).wait_recv()
        mix_on_right(c).start()
        mix_left(c).wait_recv()
        mix_on_left(c).start()
        return 0

    lax.fori_loop(0, NC, mix_second, 0)

    def b_second(c):
        b_right(c).wait_recv()
        b_on_right(c).start()
        b_left(c).wait_recv()
        b_on_left(c).start()

    for load in loads:
        load.wait()

    def finish(gate_val, up_val):
        return (gate_val / (1.0 + jnp.exp(-gate_val)) * up_val).astype(BF)

    def chunk_dots(values, mats, c):
        return [jnp.dot(values, mat[c * cw:(c + 1) * cw], preferred_element_type=F32) for mat in mats]

    def step(c, values, sums, at, store):
        g, u = chunk_dots(values, (gate_w, up_w), c)
        if c > 0:
            g = g + sums[0][at]
            u = u + sums[1][at]
        if c < NC - 1:
            sums[0][at] = g
            sums[1][at] = u
        else:
            store[at] = finish(g, u)

    def a_steps(c, part):
        a_part(c, part).wait_recv()
        per = 4 if part else 7

        def one(t, _):
            first = part * SPLIT + t * per
            values = recv_a[c, pl.ds(first, per)].reshape(per * BLOCK, cw)
            step(c, values, (acc_g, acc_u), pl.ds(pl.multiple_of(first * BLOCK, BLOCK), per * BLOCK), hid_a)
            return 0

        lax.fori_loop(0, 2, one, 0)

    def b_steps(c):
        b_on_right(c).wait_recv()
        b_on_left(c).wait_recv()

        def one(r, _):
            step(c, recv_b[c, r].reshape(NB * SLOT, cw), (bcc_g, bcc_u), r, hid_b)
            return 0

        lax.fori_loop(0, 4, one, 0)

    a_steps(0, 0)
    a_steps(0, 1)
    b_second(0)
    b_second(1)
    a_steps(1, 0)
    a_steps(1, 1)
    b_second(2)
    b_second(3)
    a_steps(2, 0)
    a_steps(2, 1)

    for c in range(NC):
        mix_on_right(c).wait_recv()
        mix_on_left(c).wait_recv()

    def project(r, _):
        start = pl.multiple_of(place(x, r) * rows, rows)
        total = None
        for c in range(NC):
            parts = chunk_dots(mix[c, r], [proj_w.at[n] for n in range(3)], c)
            total = parts if total is None else [one + two for one, two in zip(total, parts)]
        gate_b[pl.ds(start, rows)] = total[0].astype(BF)
        cin[pl.ds(start + 8, rows)] = total[1].astype(BF).astype(F32) * total[2].astype(BF).astype(F32)
        return 0

    lax.fori_loop(0, 4, project, 0)
    last = 4 * rows
    halo_next = remote(cin.at[pl.ds(last, 8)], cin.at[pl.ds(0, 8)], halo_s.at[0], halo_r.at[0], (me + 1) % 32, x)
    halo_prev = remote(cin.at[pl.ds(8, 8)], cin.at[pl.ds(last + 8, 8)], halo_s.at[1], halo_r.at[1], (me + 31) % 32, x)
    halo_next.start()
    halo_prev.start()

    b_steps(0)
    b_steps(1)
    b_steps(2)
    halo_next.wait()
    halo_prev.wait()
    cin[0:8] = cin[0:8] * jnp.where(me > 0, 1.0, 0.0)
    cin[last + 8:last + 16] = cin[last + 8:last + 16] * jnp.where(me < 31, 1.0, 0.0)
    tap = taps[...].astype(F32)
    conv = tap[0:1] * cin[7:last + 7] + tap[1:2] * cin[8:last + 8] + tap[2:3] * cin[9:last + 9]
    mixed[...] = (gate_b[...].astype(F32) * conv).astype(BF)

    a_steps(3, 0)
    b_steps(3)
    a_steps(3, 1)

    def drain(c, _):
        for copy in (
            tok_right, tok_left, tok_on_right, tok_on_left, mix_right, mix_left, mix_on_right, mix_on_left,
            b_all, b_right, b_left, b_on_right, b_on_left,
        ):
            copy(c).wait_send()
        a_part(c, 0).wait_send()
        a_part(c, 1).wait_send()
        return 0

    lax.fori_loop(0, NC, drain, 0)


def combine_kernel(
    hid_hbm, hid_b, metas, down_hbm, mixed, proj_hbm,
    out, mix_out,
    hid_a, down_w, proj_w, p_a, p_b, bh_in, bf_in, sum_b, ret_a, ret_b, w_a, w_b, p_t, th_in, tf_in, p_m, mh_in, mf_in, acc, w_t,
    bh_s, bh_r, bf_s, bf_r, b_s, b_r, a_s, a_r, th_s, th_r, tf_s, tf_r, mh_s, mh_r, mf_s, mf_r, w_sem,
):
    me = lax.axis_index("ep")
    x = lax.axis_index("tp")
    right, left = (x + 1) % 4, (x + 3) % 4
    cw = p_a.shape[3]
    rows = p_t.shape[2]
    half = rows // 2
    hb = NB // 2
    down_in = pltpu.make_async_copy(down_hbm, down_w, w_sem.at[0])
    proj_in = pltpu.make_async_copy(proj_hbm, proj_w, w_sem.at[1])
    hid_in = pltpu.make_async_copy(hid_hbm, hid_a, w_sem.at[2])
    everyone_in = greet(me, x)
    down_in.start()
    hid_in.start()
    proj_in.start()

    def cols(c):
        return pl.ds(pl.multiple_of(c * cw, cw), cw)

    def ring(buf, halves, wholes, one_s, one_r, two_s, two_r):
        size = buf.shape[2] // 2
        top = buf.shape[1] - 1
        return (
            lambda c: remote(buf.at[c, top, pl.ds(0, size)], halves.at[c, 0], one_s.at[c, 0], one_r.at[c, 0], me, right),
            lambda c: remote(buf.at[c, top, pl.ds(size, size)], halves.at[c, 1], one_s.at[c, 1], one_r.at[c, 1], me, left),
            lambda c: remote(buf.at[c, top - 1], wholes.at[c, 0], two_s.at[c, 0], two_r.at[c, 0], me, right),
            lambda c: remote(buf.at[c, top - 2], wholes.at[c, 1], two_s.at[c, 1], two_r.at[c, 1], me, left),
        )

    b_ring = ring(p_b, bh_in, bf_in, bh_s, bh_r, bf_s, bf_r)
    t_ring = ring(p_t, th_in, tf_in, th_s, th_r, tf_s, tf_r)
    m_ring = ring(p_m, mh_in, mf_in, mh_s, mh_r, mf_s, mf_r)

    def open_ring(copies, c):
        copies[0](c).start()
        copies[1](c).start()

    def pass_on(copies, buf, halves, c):
        size = buf.shape[2] // 2
        top = buf.shape[1] - 1
        copies[0](c).wait_recv()
        buf[c, top - 1, :size] = (buf[c, top - 1, :size].astype(F32) + halves[c, 0].astype(F32)).astype(BF)
        copies[2](c).start()
        copies[1](c).wait_recv()
        buf[c, top - 2, size:] = (buf[c, top - 2, size:].astype(F32) + halves[c, 1].astype(F32)).astype(BF)
        copies[3](c).start()

    def arrivals(copies, wholes, c):
        copies[2](c).wait_recv()
        copies[3](c).wait_recv()
        return wholes[c, 0].astype(F32) + wholes[c, 1].astype(F32)

    def a_all(c):
        span = pl.ds(1, NA - 1)
        return remote(p_a.at[c, span], ret_a.at[c, span], a_s.at[c], a_r.at[c], me, right)

    def b_all(c):
        return remote(sum_b.at[c], ret_b.at[c], b_s.at[c], b_r.at[c], me, right)

    def down_b(c):
        def one(r, _):
            part = jnp.dot(hid_b[r], down_w[:, cols(c)], preferred_element_type=F32)
            p_b[c, r] = part.astype(BF).reshape(NB, SLOT, cw)
            return 0

        lax.fori_loop(0, 4, one, 0)

    down_in.wait()
    down_b(0)
    everyone_in()
    open_ring(b_ring, 0)
    hid_in.wait()

    def down_a(c):
        def one(first, count):
            values = hid_a[pl.ds(pl.multiple_of(first * BLOCK, BLOCK), count * BLOCK)]
            part = jnp.dot(values, down_w[:, cols(c)], preferred_element_type=F32)
            p_a[c, pl.ds(first, count)] = part.astype(BF).reshape(count, BLOCK, cw)

        near_steps(one)
        for o in range(1, NA):
            remote(p_a.at[c, o], ret_a.at[c, o], a_s.at[c], a_r.at[c], peer(me, NEAR[o], -1), x).start()
        ret_a[c, 0] = p_a[c, 0]

    down_a(0)

    def first(c, _):
        down_b(c)
        open_ring(b_ring, c)
        return 0

    lax.fori_loop(1, NC, first, 0)
    pass_on(b_ring, p_b, bh_in, 0)

    def second(c, _):
        down_a(c)
        pass_on(b_ring, p_b, bh_in, c)
        return 0

    lax.fori_loop(1, NC, second, 0)
    proj_in.wait()

    def mixer(c, _):
        def one(r, _):
            values = mixed[pl.ds(pl.multiple_of(place(x, r) * rows, rows), rows)]
            p_m[c, r] = jnp.dot(values, proj_w[:, cols(c)], preferred_element_type=F32).astype(BF)
            return 0

        lax.fori_loop(0, 4, one, 0)
        open_ring(m_ring, c)
        return 0

    lax.fori_loop(0, NC, mixer, 0)

    for o in range(NA):
        for r in range(4):
            meta = metas[r]
            w_a[r, o] = near_rows(me, o, r, meta, meta[2:3], meta[3:4])
    for r in range(4):
        w_t[r] = w_a[r].reshape(NA * BLOCK, rows).T
    for o in range(NB):
        meta = metas[0]
        w_b[o] = far_rows(me, o, meta, meta[2:3], meta[3:4])

    def third(c, _):
        sum_b[c] = (p_b[c, 0].astype(F32) + arrivals(b_ring, bf_in, c)).astype(BF)
        for o in range(NB):
            remote(sum_b.at[c, o], ret_b.at[c, o], b_s.at[c], b_r.at[c], peer(me, FAR[o], -1), x).start()
        pass_on(m_ring, p_m, mh_in, c)
        return 0

    lax.fori_loop(0, NC, third, 0)
    over_rows = (((0,), (0,)), ((), ()))

    def weighed(r, c):
        values = ret_a[c].reshape(NA * BLOCK, cw)
        return jnp.dot(w_t[r], values, preferred_element_type=F32)

    def fourth(c, _):
        a_all(c).wait_recv()
        p_t[c, 2] = weighed(3, c).astype(BF)
        open_ring(t_ring, c)
        p_t[c, 0] = weighed(1, c).astype(BF)
        p_t[c, 1] = weighed(2, c).astype(BF)
        acc[c] = weighed(0, c)
        return 0

    lax.fori_loop(0, NC, fourth, 0)

    def fourth_on(c, _):
        pass_on(t_ring, p_t, th_in, c)
        return 0

    lax.fori_loop(0, NC, fourth_on, 0)

    def fifth(c, _):
        mix_out[:, cols(c)] = (p_m[c, 0].astype(F32) + arrivals(m_ring, mf_in, c)).astype(BF)
        return 0

    lax.fori_loop(0, NC, fifth, 0)

    def sixth(c, _):
        b_all(c).wait_recv()
        values = ret_b[c].reshape(NB * SLOT, cw)
        total = acc[c] + lax.dot_general(
            w_b[...].reshape(NB * SLOT, rows), values, over_rows, preferred_element_type=F32
        )
        out[:, cols(c)] = (total + arrivals(t_ring, tf_in, c)).astype(BF)
        return 0

    lax.fori_loop(0, NC, sixth, 0)

    def drain(c, _):
        for copy in b_ring + t_ring + m_ring + (a_all, b_all):
            copy(c).wait_send()
        return 0

    lax.fori_loop(0, NC, drain, 0)


VM = pltpu.VMEM
DMA = pltpu.SemaphoreType.DMA
PARAMS = dict(has_side_effects=True, vmem_limit_bytes=64 * 1024 * 1024 - 65536)
COST = pl.CostEstimate(flops=100_000_000_000, bytes_accessed=12_000_000, transcendentals=0)


def specs(places):
    vmem = pl.BlockSpec(memory_space=VM)
    anywhere = pl.BlockSpec(memory_space=pl.ANY)
    return [vmem if place == "v" else anywhere for place in places]


def dispatch(moe_in, moe_gain, routes, group_logits, pair_logits, gate_mat, up_mat, mix_in, mix_gain, proj_b, proj_c, proj_h, taps):
    rows, width = moe_in.shape
    hidden = gate_mat.shape[1]
    chan = proj_b.shape[1]
    cw = width // NC
    pair = DMA((NC, 2))
    single = DMA((NC,))
    return pl.pallas_call(
        dispatch_kernel,
        name="dispatch",
        out_shape=(
            jax.ShapeDtypeStruct((NA * BLOCK, hidden), BF),
            jax.ShapeDtypeStruct((4, NB * SLOT, hidden), BF),
            jax.ShapeDtypeStruct((4, 8, rows), F32),
            jax.ShapeDtypeStruct((4 * rows, chan), BF),
        ),
        in_specs=specs("avvvvaaavaaav"),
        out_specs=tuple(specs("vvvv")),
        scratch_shapes=[
            VM((rows, width), BF),
            VM((NC, 4, rows, cw), BF),
            VM((NC, 4, rows, cw), BF),
            VM((4, 8, rows), F32),
            VM((NA, BLOCK, 4 * rows), BF),
            VM((NB, SLOT, rows), BF),
            VM((NC, NA, BLOCK, cw), BF),
            VM((NC, NB, SLOT, cw), BF),
            VM((NC, NA, BLOCK, cw), BF),
            VM((NC, 4, NB, SLOT, cw), BF),
            VM((width, hidden), BF),
            VM((width, hidden), BF),
            VM((3, width, chan), BF),
            VM((NA * BLOCK, hidden), F32),
            VM((NA * BLOCK, hidden), F32),
            VM((4, NB * SLOT, hidden), F32),
            VM((4, NB * SLOT, hidden), F32),
            VM((4 * rows + 16, chan), F32),
            VM((4 * rows, chan), BF),
            pair, pair, pair, pair, pair, pair, pair, pair, single, single, pair, pair, pair, pair, pair, pair,
            DMA((3,)), DMA((3,)), DMA((2,)), DMA((2,)), DMA((7,)),
        ],
        compiler_params=pltpu.CompilerParams(collective_id=0, **PARAMS),
        cost_estimate=COST,
    )(moe_in, moe_gain, routes, group_logits, pair_logits, gate_mat, up_mat, mix_in, mix_gain, proj_b, proj_c, proj_h, taps)


def combine(hid_a, hid_b, metas, down_mat, mixed, proj_out):
    rows = metas.shape[2]
    hidden, width = down_mat.shape
    chan = proj_out.shape[0]
    cw = width // NC
    hb = NB // 2
    pair = DMA((NC, 2))
    single = DMA((NC,))
    return pl.pallas_call(
        combine_kernel,
        name="combine",
        out_shape=(jax.ShapeDtypeStruct((rows, width), BF), jax.ShapeDtypeStruct((rows, width), BF)),
        in_specs=specs("avvava"),
        out_specs=tuple(specs("vv")),
        scratch_shapes=[
            VM((NA * BLOCK, hidden), BF),
            VM((hidden, width), BF),
            VM((chan, width), BF),
            VM((NC, NA, BLOCK, cw), BF),
            VM((NC, 4, NB, SLOT, cw), BF),
            VM((NC, 2, hb, SLOT, cw), BF),
            VM((NC, 2, NB, SLOT, cw), BF),
            VM((NC, NB, SLOT, cw), BF),
            VM((NC, NA, BLOCK, cw), BF),
            VM((NC, NB, SLOT, cw), BF),
            VM((4, NA, BLOCK, rows), BF),
            VM((NB, SLOT, rows), BF),
            VM((NC, 3, rows, cw), BF),
            VM((NC, 2, rows // 2, cw), BF),
            VM((NC, 2, rows, cw), BF),
            VM((NC, 4, rows, cw), BF),
            VM((NC, 2, rows // 2, cw), BF),
            VM((NC, 2, rows, cw), BF),
            VM((NC, rows, cw), F32),
            VM((4, rows, NA * BLOCK), BF),
            pair, pair, pair, pair, single, single, single, single,
            pair, pair, pair, pair, pair, pair, pair, pair, DMA((3,)),
        ],
        compiler_params=pltpu.CompilerParams(collective_id=1, **PARAMS),
        cost_estimate=COST,
    )(hid_a, hid_b, metas, down_mat, mixed, proj_out)


def body(
    mix_in, mix_gain, proj_b, proj_c, proj_h, conv_taps, proj_out,
    moe_in, moe_gain, routes, group_logits, pair_logits, expert_gate, expert_up, expert_down,
):
    hid_a, hid_b, metas, mixed = dispatch(
        moe_in, moe_gain[None, :], routes.T, group_logits.T, pair_logits.T, expert_gate[0], expert_up[0],
        mix_in, mix_gain[None, :], proj_b, proj_c, proj_h, conv_taps,
    )
    moe_out, mix_out = combine(hid_a, hid_b, metas, expert_down[0], mixed, proj_out)
    return (mix_out, moe_out)


def solution(mesh):
    in_specs = (
        P(("ep", "tp"), None), P(), P(None, "tp"), P(None, "tp"), P(None, "tp"), P(None, "tp"), P("tp", None),
        P(("ep", "tp"), None), P(), P(("ep", "tp"), None), P(("ep", "tp"), None), P(("ep", "tp"), None),
        P("ep", None, "tp"), P("ep", None, "tp"), P("ep", "tp", None),
    )
    out_specs = (P(("ep", "tp"), None), P(("ep", "tp"), None))
    return jax.shard_map(body, mesh=mesh, in_specs=in_specs, out_specs=out_specs, check_vma=False)
```
